32 devices in a mesh: sp: 8 (over z, x), tp: 4 (over y, core).
Axes of the slice: x: 2, y: 2, z: 4, core: 2. Of those that a mesh axis runs over, the one named last changes fastest.
Arguments:
- latent: bfloat16 [2, 4096, 2048], P(None, ('sp', 'tp')), may hold values from -6 to 6
- context: bfloat16 [2, 512, 2048], P(None, 'sp'), may hold values from -6 to 6
- cond: bfloat16 [2, 2048], replicated, may hold values from -6 to 6
- ctx_cond: bfloat16 [2048], replicated, may hold values from -6 to 6
- w_shift: bfloat16 [2048, 2048], P('sp', 'tp'), may hold values from -0.125 to 0.125
- w_scale: bfloat16 [2048, 2048], P('sp', 'tp'), may hold values from -0.125 to 0.125
- w_gate: bfloat16 [2048, 2048], P('sp', 'tp'), may hold values from -0.125 to 0.125
- norm_gain: float32 [2048], replicated, may hold values from 0.1 to 1.9
- w_query: bfloat16 [2048, 2048], P(None, 'tp'), may hold values from -1.08275726 to 1.08275726
- w_key: bfloat16 [2048, 2048], P(None, 'tp'), may hold values from -0.090598056 to 0.090598056
- w_value: bfloat16 [2048, 2048], P(None, 'tp'), may hold values from -0.125 to 0.125
- w_out: bfloat16 [2048, 2048], P('tp'), may hold values from -1.5 to 1.5
- rel_bias: float32 [32, 15, 31], P('tp'), may hold values from -4 to 4
- ctx_bias: float32 [32], P('tp'), may hold values from -3.5 to -2
Outputs:
- mixed: bfloat16 [2, 4096, 2048], P(None, ('sp', 'tp'))
The draws below stay inside these ranges and needn't reach their ends.
All inputs are finite; a program needn't handle non-finite values.
Results may differ from the reference program's by a relative error of at most 0.0154.
Values may be sent and summed in bfloat16 or wider, within the bound.
A program may use at most 128 MiB of HBM per device.

```python
import jax
import jax.numpy as jnp
from jax import lax

D = 2048
HEADS = 32
HEAD_DIM = 64
GRID_W = 64
WIN_ROWS = 8
WIN_COLS = 16
SAMPLES = 2
ROWS = 64
TOKENS = 4096
CTX = 512
N_TP = 4


def shared_keys(key):
    base = jax.random.normal(jax.random.fold_in(key, 11), (D, D), jnp.float32)
    return jnp.clip(base, -4.0, 4.0) * D ** (-0.5)


def draw_w_key(key, part):
    return shared_keys(key).astype(jnp.bfloat16)


def draw_w_query(key, part):
    own = jax.random.normal(jax.random.fold_in(key, 12), (D, D), jnp.float32)
    own = jnp.clip(own, -4.0, 4.0) * D ** (-0.5)
    return own.astype(jnp.bfloat16)


def levels(own_key, extent, pieces, smallest, high):
    loudness, own = 1.0, jax.random.fold_in(own_key, 6)
    for axis_at, parts in pieces:
        steps = jnp.exp(jax.random.uniform(jax.random.fold_in(own, axis_at), (parts,), jnp.float32, smallest / len(pieces), high / len(pieces)))
        loudness = loudness * jnp.repeat(steps, extent[axis_at] // parts).reshape([-1 if axis == axis_at else 1 for axis in range(len(extent))])
    return loudness


def noise(stream_key, extent, width, limit, shards=(), kind=jnp.bfloat16):
    entries = jax.random.normal(stream_key, extent, jnp.float32) * width
    if len(shards) > 0:
        entries = levels(stream_key, extent, shards, -0.22, 0.18) * entries
    return jnp.clip(entries, min=-limit, max=limit).astype(kind)


def setup_inputs(seed: int = 0) -> dict:
    key_list = jax.random.split(jax.random.key(seed), 15)
    return {
        "latent": noise(key_list[0], (SAMPLES, TOKENS, D), 1.0, 6.0, ((1, 32),)),
        "context": noise(key_list[1], (SAMPLES, CTX, D), 1.0, 6.0, ((1, 8),)),
        "cond": noise(key_list[2], (SAMPLES, D), 1.0, 6.0),
        "ctx_cond": noise(key_list[3], (D,), 1.0, 6.0),
        "w_shift": noise(key_list[4], (D, D), D ** -0.5, 0.125, ((0, 8), (1, 4))),
        "w_scale": noise(key_list[5], (D, D), D ** -0.5, 0.125, ((0, 8), (1, 4))),
        "w_gate": noise(key_list[6], (D, D), D ** -0.5, 0.125, ((0, 8), (1, 4))),
        "norm_gain": jnp.clip(1.0 + 0.18 * jax.random.normal(key_list[7], (D,), jnp.float32), 0.1, 1.9),
        "w_query": draw_w_query(jax.random.fold_in(key_list[14], 71), 0),
        "w_key": draw_w_key(jax.random.fold_in(key_list[14], 71), 0),
        "w_value": noise(key_list[10], (D, D), D ** -0.5, 0.125, ((1, 4),)),
        "w_out": noise(key_list[11], (D, D), 16 ** -0.5, 1.5, ((0, 4),)),
        "rel_bias": noise(key_list[12], (HEADS, 2 * WIN_ROWS - 1, 2 * WIN_COLS - 1), 1.0, 4.0, ((0, 4),), jnp.float32),
        "ctx_bias": jnp.clip(-3.5 + 1.5 * jax.random.uniform(key_list[13], (HEADS,), jnp.float32) ** levels(key_list[13], (HEADS,), ((0, 4),), -0.2, 0.2), -3.5, -2.0),
    }


EPSILON = 1e-06

def modulate_rows(rows, gain, shift, scale):
    floats = rows.astype(jnp.float32)
    inverse = lax.rsqrt(lax.optimization_barrier(jnp.mean(floats * floats, axis=-1, keepdims=True)) + EPSILON)
    return (floats * inverse * gain * (1.0 + scale) + shift).astype(jnp.bfloat16)

def project(rows, weight):
    return jnp.dot(rows, weight, preferred_element_type=jnp.float32).astype(jnp.bfloat16)

def reference(latent, context, cond, ctx_cond, w_shift, w_scale, w_gate, norm_gain, w_query, w_key, w_value, w_out, rel_bias, ctx_bias):
    ada = jax.nn.silu(cond.astype(jnp.float32)).astype(jnp.bfloat16)
    ada_ctx = jax.nn.silu(ctx_cond.astype(jnp.float32)).astype(jnp.bfloat16)[None, :]
    shift = jnp.dot(ada, w_shift, preferred_element_type=jnp.float32)
    scale = jnp.dot(ada, w_scale, preferred_element_type=jnp.float32)
    gate = jnp.dot(ada, w_gate, preferred_element_type=jnp.float32)
    ctx_shift = jnp.dot(ada_ctx, w_shift, preferred_element_type=jnp.float32)[0]
    ctx_scale = jnp.dot(ada_ctx, w_scale, preferred_element_type=jnp.float32)[0]
    hidden = modulate_rows(latent, norm_gain, shift[:, None, :], scale[:, None, :])
    ctx_hidden = modulate_rows(context, norm_gain, ctx_shift, ctx_scale)
    query = project(hidden, w_query).reshape(SAMPLES, ROWS, GRID_W, HEADS, HEAD_DIM)
    key = project(hidden, w_key).reshape(SAMPLES, ROWS, GRID_W, HEADS, HEAD_DIM)
    value = project(hidden, w_value).reshape(SAMPLES, ROWS, GRID_W, HEADS, HEAD_DIM)
    ctx_key = project(ctx_hidden, w_key).reshape(SAMPLES, CTX, HEADS, HEAD_DIM).astype(jnp.float32)
    ctx_value = project(ctx_hidden, w_value).reshape(SAMPLES, CTX, HEADS, HEAD_DIM).astype(jnp.float32)
    factor = HEAD_DIM ** (-0.5)
    columns = jnp.arange(GRID_W, dtype=jnp.int32)
    col_start = jnp.clip(columns - WIN_COLS // 2, 0, GRID_W - WIN_COLS)
    col_mask = (columns[None, :] >= col_start[:, None]) & (columns[None, :] < col_start[:, None] + WIN_COLS)
    col_index = jnp.clip(columns[None, :] - columns[:, None] + WIN_COLS - 1, 0, 2 * WIN_COLS - 2)

    def one_row(row):
        first = jnp.clip(row - WIN_ROWS // 2, 0, ROWS - WIN_ROWS).astype(jnp.int32)
        query_row = lax.dynamic_index_in_dim(query, row, axis=1, keepdims=False).astype(jnp.float32)
        key_rows = lax.dynamic_slice_in_dim(key, first, WIN_ROWS, axis=1).astype(jnp.float32)
        value_rows = lax.dynamic_slice_in_dim(value, first, WIN_ROWS, axis=1).astype(jnp.float32)
        row_index = first + jnp.arange(WIN_ROWS, dtype=jnp.int32) - row + WIN_ROWS - 1
        bias = rel_bias[:, row_index][:, :, col_index]
        near = jnp.einsum('sqhd,siwhd->shqiw', query_row, key_rows) * factor + bias.transpose(0, 2, 1, 3)[None]
        near = jnp.where(col_mask[None, None, :, None, :], near, -jnp.inf).reshape(SAMPLES, HEADS, GRID_W, WIN_ROWS * GRID_W)
        far = jnp.einsum('sqhd,schd->shqc', query_row, ctx_key) * factor + ctx_bias[None, :, None, None]
        top = jnp.maximum(lax.optimization_barrier(jnp.max(near, axis=-1)), lax.optimization_barrier(jnp.max(far, axis=-1)))[..., None]
        near_exp = jnp.exp(near - top)
        far_exp = jnp.exp(far - top)
        total = lax.optimization_barrier(jnp.sum(near_exp, axis=-1, keepdims=True)) + lax.optimization_barrier(jnp.sum(far_exp, axis=-1, keepdims=True))
        near_weight = (near_exp / total).astype(jnp.bfloat16).astype(jnp.float32)
        far_weight = (far_exp / total).astype(jnp.bfloat16).astype(jnp.float32)
        near_weight = near_weight.reshape(SAMPLES, HEADS, GRID_W, WIN_ROWS, GRID_W)
        mixed = jnp.einsum('shqiw,siwhd->sqhd', near_weight, value_rows) + jnp.einsum('shqc,schd->sqhd', far_weight, ctx_value)
        return mixed.astype(jnp.bfloat16)
    attended = lax.map(one_row, jnp.arange(ROWS, dtype=jnp.int32))
    attended = attended.transpose(1, 0, 2, 3, 4).reshape(SAMPLES, TOKENS, D)
    group = D // N_TP
    update = jnp.zeros((SAMPLES, TOKENS, D), jnp.float32)
    for index in range(N_TP):
        part = jnp.dot(attended[..., index * group:(index + 1) * group], w_out[index * group:(index + 1) * group], preferred_element_type=jnp.float32).astype(jnp.bfloat16)
        part = lax.optimization_barrier(part)
        update = update + part.astype(jnp.float32)
    mixed_out = latent.astype(jnp.float32) + gate[:, None, :] * update
    return mixed_out.astype(jnp.bfloat16)
```

```python
import jax
import jax.numpy as jnp
from jax import lax
from jax.experimental import pallas as pl
from jax.experimental.pallas import tpu as pltpu
from jax.sharding import PartitionSpec as P

HEAD_DIM = 64
GRID_W = 64
WIN_ROWS = 8
WIN_COLS = 16


EPSILON = 1e-06


def extended(shard, sides, width):
    for axis, dim in sides:
        size, length = (lax.axis_size(axis), shard.shape[dim])
        up = [(i, (i + 1) % size) for i in range(size - 1)]
        down = [(j, i) for i, j in up]
        last = lax.slice_in_dim(shard, length - width, length, axis=dim)
        first = lax.slice_in_dim(shard, 0, width, axis=dim)
        before = lax.ppermute(last, axis, up)
        after = lax.ppermute(first, axis, down)
        shard = jnp.concatenate([before, shard, after], axis=dim)
    return shard


def silu_rows(values):
    return jax.nn.silu(values.astype(jnp.float32)).astype(jnp.bfloat16)


def modulate_rows(rows, gain, shift, scale):
    floats = rows.astype(jnp.float32)
    inverse = lax.rsqrt(jnp.mean(floats * floats, axis=-1, keepdims=True) + EPSILON)
    return (floats * inverse * gain * (1.0 + scale) + shift).astype(jnp.bfloat16)

LOG2E = 1.4426950408889634


def attention_kernel(bias_ref, far_ref, q_ref, k_ref, v_ref, ck_ref, cv_ref, out_ref, table):
    pair = pl.program_id(0)
    rows_dev = q_ref.shape[1]
    padded = k_ref.shape[1]
    span = 2 * WIN_COLS
    half = WIN_COLS // 2
    reach = WIN_ROWS // 2
    nq, nk = rows_dev * WIN_COLS, padded * span
    lanes = 2 * HEAD_DIM

    @pl.when(pl.program_id(1) == 0)
    def _():
        sp = lax.axis_index("sp")
        rows_all = rows_dev * lax.axis_size("sp")
        at = lax.broadcasted_iota(jnp.int32, (WIN_COLS, nk), 1)
        p = lax.broadcasted_iota(jnp.int32, (WIN_COLS, nk), 0)
        key_row = sp * rows_dev - reach + at // span
        k = at % span
        inner = (k - p >= 0) & (k - p < WIN_COLS)
        edge = (p < half) == (k < WIN_COLS)
        for r in range(rows_dev):
            row = sp * rows_dev + r
            first = jnp.clip(row - reach, 0, rows_all - WIN_ROWS)
            inside = (key_row >= first) & (key_row < first + WIN_ROWS)
            shift = span * (r + reach - WIN_ROWS + 1) - half + 1
            for h in range(2):
                line = jnp.broadcast_to(bias_ref[0, h : h + 1, :], (WIN_COLS, nk))
                line = pltpu.roll(line, shift % nk, 1, stride=1, stride_axis=0) * LOG2E
                at_rows = pl.ds(r * WIN_COLS, WIN_COLS)
                table[h, 0, at_rows, :] = jnp.where(inside & edge, line, -jnp.inf)
                table[h, 1, at_rows, :] = jnp.where(inside & inner, line, -jnp.inf)

    factor = HEAD_DIM ** (-0.5) * LOG2E
    ck = ck_ref[0]
    ctx_count = ck.shape[0]
    cv = jnp.concatenate([cv_ref[0], jnp.ones((ctx_count, lanes), jnp.bfloat16)], axis=1)
    ones = jnp.ones((nk, lanes), jnp.bfloat16)
    low = lax.broadcasted_iota(jnp.int32, (nq, lanes), 1) < HEAD_DIM
    contract = (((1,), (1,)), ((), ()))
    for block in range(GRID_W // WIN_COLS):
        q = q_ref[0, :, WIN_COLS * block : WIN_COLS * (block + 1), :].reshape(nq, lanes)

        def keys(ref):
            if block == 0:
                got = jnp.concatenate([ref[0, :, GRID_W - WIN_COLS :, :], ref[0, :, :WIN_COLS, :]], 1)
            else:
                got = ref[0, :, WIN_COLS * (block - 1) : WIN_COLS * (block + 1), :]
            return got.reshape(nk, lanes)

        k = keys(k_ref)
        v = jnp.concatenate([keys(v_ref), ones], axis=1)
        halves = []
        for h in range(2):
            mine = low if h == 0 else jnp.logical_not(low)
            one = jnp.where(mine, q, jnp.zeros_like(q))
            near = lax.dot_general(one, k, contract, preferred_element_type=jnp.float32)
            near = near * factor + table[h, min(block, 1)]
            far = lax.dot_general(one, ck, contract, preferred_element_type=jnp.float32)
            far = far * factor + far_ref[2 * pair + h] * LOG2E
            top = jnp.maximum(
                jnp.max(near, axis=-1, keepdims=True), jnp.max(far, axis=-1, keepdims=True)
            )
            near = jnp.exp2(near - top).astype(jnp.bfloat16)
            far = jnp.exp2(far - top).astype(jnp.bfloat16)
            got = jnp.dot(near, v, preferred_element_type=jnp.float32) + jnp.dot(
                far, cv, preferred_element_type=jnp.float32
            )
            halves.append(got[:, :lanes] / got[:, lanes:])
        got = jnp.where(low, halves[0], halves[1]).astype(jnp.bfloat16)
        out_ref[0, :, WIN_COLS * block : WIN_COLS * (block + 1), :] = got.reshape(
            rows_dev, WIN_COLS, lanes
        )


def attention(query, pair, ctx_pair, rel_bias, ctx_bias):
    samples, rows_dev, _, cols = query.shape
    padded, ctx_count = pair.shape[1], ctx_pair.shape[1]
    heads = cols // HEAD_DIM
    lanes = 2 * HEAD_DIM
    pairs = cols // lanes
    nq, nk = rows_dev * WIN_COLS, padded * 2 * WIN_COLS
    flat = jnp.pad(rel_bias, ((0, 0), (0, 1), (0, 1))).reshape(heads, -1)
    flat = jnp.pad(flat, ((0, 0), (0, nk - flat.shape[1]))).reshape(pairs, 2, nk)
    token = lambda at: pl.BlockSpec((1, padded, GRID_W, lanes), lambda p, s: (s, 0, 0, p + at))
    far = lambda at: pl.BlockSpec((1, ctx_count, lanes), lambda p, s: (s, 0, p + at))
    own = pl.BlockSpec((1, rows_dev, GRID_W, lanes), lambda p, s: (s, 0, 0, p))
    scores = samples * heads * 4 * nq * (nk + ctx_count)
    return pl.pallas_call(
        attention_kernel,
        grid=(pairs, samples),
        out_shape=jax.ShapeDtypeStruct(query.shape, jnp.bfloat16),
        in_specs=[
            pl.BlockSpec((1, 2, nk), lambda p, s: (p, 0, 0)),
            pl.BlockSpec(memory_space=pltpu.SMEM),
            own,
            token(0),
            token(pairs),
            far(0),
            far(pairs),
        ],
        out_specs=own,
        scratch_shapes=[pltpu.VMEM((2, 2, nq, nk), jnp.float32)],
        cost_estimate=pl.CostEstimate(
            flops=scores * 512, bytes_accessed=8 * query.size * 2, transcendentals=scores
        ),
    )(flat, ctx_bias, query, pair, pair, ctx_pair, ctx_pair)


def on_device(
    latent,
    context,
    cond,
    ctx_cond,
    w_shift,
    w_scale,
    w_gate,
    norm_gain,
    w_query,
    w_key,
    w_value,
    w_out,
    rel_bias,
    ctx_bias,
):
    samples = latent.shape[0]
    rows_sp = w_shift.shape[0]
    local_cols = w_shift.shape[1]
    sp_index = lax.axis_index("sp")
    ada = silu_rows(jnp.concatenate([cond, ctx_cond[None, :]], axis=0))
    ada_rows = lax.dynamic_slice_in_dim(ada, sp_index * rows_sp, rows_sp, 1)
    partial_value = jnp.stack(
        [
            jnp.dot(ada_rows, weight, preferred_element_type=jnp.float32)
            for weight in (w_shift, w_scale, w_gate)
        ]
    )
    summed = lax.psum(partial_value, "sp")
    modulation = lax.all_gather(summed, "tp", axis=2, tiled=True)
    hidden = modulate_rows(
        latent, norm_gain, modulation[0, :samples, None, :], modulation[1, :samples, None, :]
    )
    w_triple = jnp.concatenate([w_query, w_key, w_value], axis=1)
    triple = jnp.dot(
        lax.all_gather(hidden, "tp", axis=1, tiled=True),
        w_triple,
        preferred_element_type=jnp.float32,
    ).astype(jnp.bfloat16)
    ctx_hidden = modulate_rows(context, norm_gain, modulation[0, samples], modulation[1, samples])
    w_pair = jnp.concatenate([w_key, w_value], axis=1)
    own_pair = jnp.dot(ctx_hidden, w_pair, preferred_element_type=jnp.float32).astype(jnp.bfloat16)
    ctx_pair = lax.all_gather(own_pair, "sp", axis=1, tiled=True)
    heads = local_cols // HEAD_DIM
    tokens_sp = triple.shape[1]
    rows_dev = tokens_sp // GRID_W
    rows_all = rows_dev * lax.axis_size("sp")
    reach = WIN_ROWS // 2
    query = triple[..., :local_cols].reshape(samples, rows_dev, GRID_W, local_cols)
    pair = triple[..., local_cols:].reshape(samples, rows_dev, GRID_W, 2 * local_cols)
    padded_pair = extended(pair, (("sp", 1),), reach)
    half = WIN_COLS // 2
    rolled = jnp.roll(query, half, axis=2)
    mixed = attention(rolled, padded_pair, ctx_pair, rel_bias, ctx_bias)
    attended = jnp.roll(mixed, -half, axis=2).reshape(samples, tokens_sp, local_cols)
    attended = attended.transpose(1, 0, 2)
    update = lax.psum_scatter(
        jnp.einsum("tsc,cd->tsd", attended, w_out, preferred_element_type=jnp.float32).astype(
            jnp.bfloat16
        ),
        "tp",
        scatter_dimension=0,
        tiled=True,
    ).astype(jnp.float32)
    gate = modulation[2, :samples, None, :]
    result = latent.astype(jnp.float32) + gate * update.transpose(1, 0, 2)
    return result.astype(jnp.bfloat16)


def solution(mesh):
    return jax.shard_map(
        on_device,
        mesh=mesh,
        in_specs=(
            P(None, ("sp", "tp"), None),
            P(None, "sp", None),
            P(),
            P(),
            P("sp", "tp"),
            P("sp", "tp"),
            P("sp", "tp"),
            P(),
            P(None, "tp"),
            P(None, "tp"),
            P(None, "tp"),
            P("tp", None),
            P("tp", None, None),
            P("tp"),
        ),
        out_specs=P(None, ("sp", "tp"), None),
        check_vma=False,
    )
```

```python
import jax
import jax.numpy as jnp
from jax import lax
from jax.experimental import pallas as pl
from jax.experimental.pallas import tpu as pltpu
from jax.sharding import PartitionSpec as P

HEAD_DIM = 64
GRID_W = 64
WIN_ROWS = 8
WIN_COLS = 16


EPSILON = 1e-06


def extended(shard, sides, width):
    for axis, dim in sides:
        size, length = (lax.axis_size(axis), shard.shape[dim])
        up = [(i, (i + 1) % size) for i in range(size - 1)]
        down = [(j, i) for i, j in up]
        last = lax.slice_in_dim(shard, length - width, length, axis=dim)
        first = lax.slice_in_dim(shard, 0, width, axis=dim)
        before = lax.ppermute(last, axis, up)
        after = lax.ppermute(first, axis, down)
        shard = jnp.concatenate([before, shard, after], axis=dim)
    return shard


def silu_rows(values):
    return jax.nn.silu(values.astype(jnp.float32)).astype(jnp.bfloat16)


def modulate_rows(rows, gain, shift, scale):
    floats = rows.astype(jnp.float32)
    inverse = lax.rsqrt(jnp.mean(floats * floats, axis=-1, keepdims=True) + EPSILON)
    return (floats * inverse * gain * (1.0 + scale) + shift).astype(jnp.bfloat16)

LOG2E = 1.4426950408889634


def attention_kernel(bias_ref, far_ref, q_ref, k_ref, v_ref, ck_ref, cv_ref, out_ref, table):
    pair = pl.program_id(0)
    rows_dev = q_ref.shape[1]
    padded = k_ref.shape[1]
    span = 2 * WIN_COLS
    half = WIN_COLS // 2
    reach = WIN_ROWS // 2
    nq, nk = rows_dev * WIN_COLS, padded * span
    lanes = 2 * HEAD_DIM

    @pl.when(pl.program_id(1) == 0)
    def _():
        sp = lax.axis_index("sp")
        rows_all = rows_dev * lax.axis_size("sp")
        at = lax.broadcasted_iota(jnp.int32, (WIN_COLS, nk), 1)
        p = lax.broadcasted_iota(jnp.int32, (WIN_COLS, nk), 0)
        key_row = sp * rows_dev - reach + at // span
        k = at % span
        inner = (k - p >= 0) & (k - p < WIN_COLS)
        edge = (p < half) == (k < WIN_COLS)
        for r in range(rows_dev):
            row = sp * rows_dev + r
            first = jnp.clip(row - reach, 0, rows_all - WIN_ROWS)
            inside = (key_row >= first) & (key_row < first + WIN_ROWS)
            shift = span * (r + reach - WIN_ROWS + 1) - half + 1
            for h in range(2):
                line = jnp.broadcast_to(bias_ref[0, h : h + 1, :], (WIN_COLS, nk))
                line = pltpu.roll(line, shift % nk, 1, stride=1, stride_axis=0) * LOG2E
                at_rows = pl.ds(r * WIN_COLS, WIN_COLS)
                table[h, 0, at_rows, :] = jnp.where(inside & edge, line, -jnp.inf)
                table[h, 1, at_rows, :] = jnp.where(inside & inner, line, -jnp.inf)

    factor = HEAD_DIM ** (-0.5) * LOG2E
    ck = ck_ref[0]
    ctx_count = ck.shape[0]
    cv = jnp.concatenate([cv_ref[0], jnp.ones((ctx_count, lanes), jnp.bfloat16)], axis=1)
    ones = jnp.ones((nk, lanes), jnp.bfloat16)
    low = lax.broadcasted_iota(jnp.int32, (nq, lanes), 1) < HEAD_DIM
    contract = (((1,), (1,)), ((), ()))
    for block in range(GRID_W // WIN_COLS):
        q = q_ref[0, :, WIN_COLS * block : WIN_COLS * (block + 1), :].reshape(nq, lanes)

        def keys(ref):
            if block == 0:
                got = jnp.concatenate([ref[0, :, GRID_W - WIN_COLS :, :], ref[0, :, :WIN_COLS, :]], 1)
            else:
                got = ref[0, :, WIN_COLS * (block - 1) : WIN_COLS * (block + 1), :]
            return got.reshape(nk, lanes)

        k = keys(k_ref)
        v = jnp.concatenate([keys(v_ref), ones], axis=1)
        halves = []
        for h in range(2):
            mine = low if h == 0 else jnp.logical_not(low)
            one = jnp.where(mine, q, jnp.zeros_like(q))
            near = lax.dot_general(one, k, contract, preferred_element_type=jnp.float32)
            near = near * factor + table[h, min(block, 1)]
            far = lax.dot_general(one, ck, contract, preferred_element_type=jnp.float32)
            far = far * factor + far_ref[2 * pair + h] * LOG2E
            top = jnp.maximum(
                jnp.max(near, axis=-1, keepdims=True), jnp.max(far, axis=-1, keepdims=True)
            )
            near = jnp.exp2(near - top).astype(jnp.bfloat16)
            far = jnp.exp2(far - top).astype(jnp.bfloat16)
            got = jnp.dot(near, v, preferred_element_type=jnp.float32) + jnp.dot(
                far, cv, preferred_element_type=jnp.float32
            )
            halves.append(got[:, :lanes] / got[:, lanes:])
        got = jnp.where(low, halves[0], halves[1]).astype(jnp.bfloat16)
        out_ref[0, :, WIN_COLS * block : WIN_COLS * (block + 1), :] = got.reshape(
            rows_dev, WIN_COLS, lanes
        )


def attention(query, pair, ctx_pair, rel_bias, ctx_bias):
    samples, rows_dev, _, cols = query.shape
    padded, ctx_count = pair.shape[1], ctx_pair.shape[1]
    heads = cols // HEAD_DIM
    lanes = 2 * HEAD_DIM
    pairs = cols // lanes
    nq, nk = rows_dev * WIN_COLS, padded * 2 * WIN_COLS
    flat = jnp.pad(rel_bias, ((0, 0), (0, 1), (0, 1))).reshape(heads, -1)
    flat = jnp.pad(flat, ((0, 0), (0, nk - flat.shape[1]))).reshape(pairs, 2, nk)
    token = lambda at: pl.BlockSpec((1, padded, GRID_W, lanes), lambda p, s: (s, 0, 0, p + at))
    far = lambda at: pl.BlockSpec((1, ctx_count, lanes), lambda p, s: (s, 0, p + at))
    own = pl.BlockSpec((1, rows_dev, GRID_W, lanes), lambda p, s: (s, 0, 0, p))
    scores = samples * heads * 4 * nq * (nk + ctx_count)
    return pl.pallas_call(
        attention_kernel,
        grid=(pairs, samples),
        out_shape=jax.ShapeDtypeStruct(query.shape, jnp.bfloat16),
        in_specs=[
            pl.BlockSpec((1, 2, nk), lambda p, s: (p, 0, 0)),
            pl.BlockSpec(memory_space=pltpu.SMEM),
            own,
            token(0),
            token(pairs),
            far(0),
            far(pairs),
        ],
        out_specs=own,
        scratch_shapes=[pltpu.VMEM((2, 2, nq, nk), jnp.float32)],
        cost_estimate=pl.CostEstimate(
            flops=scores * 512, bytes_accessed=8 * query.size * 2, transcendentals=scores
        ),
    )(flat, ctx_bias, query, pair, pair, ctx_pair, ctx_pair)


def on_device(
    latent,
    context,
    cond,
    ctx_cond,
    w_shift,
    w_scale,
    w_gate,
    norm_gain,
    w_query,
    w_key,
    w_value,
    w_out,
    rel_bias,
    ctx_bias,
):
    samples = latent.shape[0]
    rows_sp = w_shift.shape[0]
    local_cols = w_shift.shape[1]
    sp_index = lax.axis_index("sp")
    ada = silu_rows(jnp.concatenate([cond, ctx_cond[None, :]], axis=0))
    ada_rows = lax.dynamic_slice_in_dim(ada, sp_index * rows_sp, rows_sp, 1)
    partial_value = jnp.stack(
        [
            jnp.dot(ada_rows, weight, preferred_element_type=jnp.float32)
            for weight in (w_shift, w_scale, w_gate)
        ]
    )
    summed = lax.psum(partial_value, "sp")
    modulation = lax.all_gather(summed, "tp", axis=2, tiled=True)
    hidden = modulate_rows(
        latent, norm_gain, modulation[0, :samples, None, :], modulation[1, :samples, None, :]
    )
    w_triple = jnp.concatenate([w_query, w_key, w_value], axis=1)
    triple = jnp.dot(
        lax.all_gather(hidden, "tp", axis=1, tiled=True),
        w_triple,
        preferred_element_type=jnp.float32,
    ).astype(jnp.bfloat16)
    ctx_hidden = modulate_rows(context, norm_gain, modulation[0, samples], modulation[1, samples])
    w_pair = jnp.concatenate([w_key, w_value], axis=1)
    own_pair = jnp.dot(ctx_hidden, w_pair, preferred_element_type=jnp.float32).astype(jnp.bfloat16)
    ctx_pair = lax.all_gather(own_pair, "sp", axis=1, tiled=True)
    heads = local_cols // HEAD_DIM
    tokens_sp = triple.shape[1]
    rows_dev = tokens_sp // GRID_W
    rows_all = rows_dev * lax.axis_size("sp")
    reach = WIN_ROWS // 2
    query = triple[..., :local_cols].reshape(samples, rows_dev, GRID_W, local_cols)
    pair = triple[..., local_cols:].reshape(samples, rows_dev, GRID_W, 2 * local_cols)
    padded_pair = extended(pair, (("sp", 1),), reach)
    half = WIN_COLS // 2
    rolled = jnp.roll(query, half, axis=2)
    mixed = attention(rolled, padded_pair, ctx_pair, rel_bias, ctx_bias)
    attended = jnp.roll(mixed, -half, axis=2).reshape(samples, tokens_sp, local_cols)
    attended = attended.transpose(1, 0, 2)
    update = lax.psum_scatter(
        jnp.einsum("tsc,cd->tsd", attended, w_out, preferred_element_type=jnp.float32).astype(
            jnp.bfloat16
        ),
        "tp",
        scatter_dimension=0,
        tiled=True,
    ).astype(jnp.float32)
    gate = modulation[2, :samples, None, :]
    result = latent.astype(jnp.float32) + gate * update.transpose(1, 0, 2)
    return result.astype(jnp.bfloat16)


MESH = pl.DeviceIdType.MESH


def entry_barrier(peers):
    barrier = pltpu.get_barrier_semaphore()
    for device, there in peers:
        @pl.when(there)
        def _():
            pl.semaphore_signal(barrier, inc=1, device_id=device, device_id_type=MESH)
    pl.semaphore_wait(barrier, sum(jnp.where(there, 1, 0) for _, there in peers))


def modulation_kernel(ada_ref, a_ref, b_ref, c_ref, out_ref, part, got, total, full, s1, r1, s2, r2):
    sp, tp = lax.axis_index("sp"), lax.axis_index("tp")
    n_sp, n_tp = lax.axis_size("sp"), lax.axis_size("tp")
    over_sp = [lax.rem(sp + k, n_sp) for k in range(1, n_sp)]
    over_tp = [lax.rem(tp + k, n_tp) for k in range(1, n_tp)]
    entry_barrier([((p, tp), sp >= 0) for p in over_sp] + [((sp, p), sp >= 0) for p in over_tp])
    for at, weight in enumerate((a_ref, b_ref, c_ref)):
        value = jnp.dot(ada_ref[...], weight[...], preferred_element_type=jnp.float32)
        part[8 * at : 8 * at + 8, :] = value[:8]

    def first(k, peer):
        return pltpu.make_async_remote_copy(
            src_ref=part, dst_ref=got.at[k], send_sem=s1.at[k], recv_sem=r1.at[k],
            device_id=(peer, tp), device_id_type=MESH,
        )

    def second(k, peer):
        return pltpu.make_async_remote_copy(
            src_ref=total, dst_ref=full.at[k], send_sem=s2.at[k], recv_sem=r2.at[k],
            device_id=(sp, peer), device_id_type=MESH,
        )

    copies = [first(k, peer) for k, peer in enumerate(over_sp)]
    for copy in copies:
        copy.start()
    value = part[...]
    for k, copy in enumerate(copies):
        copy.wait()
        value = value + got[k]
    total[...] = value
    copies = [second(k, peer) for k, peer in enumerate(over_tp)]
    for copy in copies:
        copy.start()
    out_ref[0] = value
    for k, copy in enumerate(copies):
        copy.wait()
        out_ref[k + 1] = full[k]


def modulation_vectors(ada_rows, weights):
    n_sp, n_tp = lax.axis_size("sp"), lax.axis_size("tp")
    cols = weights[0].shape[1]
    block = (24, cols)
    ada_rows = jnp.pad(ada_rows, ((0, 16 - ada_rows.shape[0]), (0, 0)))
    got = pl.pallas_call(
        modulation_kernel,
        out_shape=jax.ShapeDtypeStruct((n_tp,) + block, jnp.float32),
        in_specs=[pl.BlockSpec(memory_space=pltpu.VMEM)] * 4,
        out_specs=pl.BlockSpec(memory_space=pltpu.VMEM),
        scratch_shapes=[
            pltpu.VMEM(block, jnp.float32),
            pltpu.VMEM((n_sp - 1,) + block, jnp.float32),
            pltpu.VMEM(block, jnp.float32),
            pltpu.VMEM((n_tp - 1,) + block, jnp.float32),
            pltpu.SemaphoreType.DMA((n_sp - 1,)),
            pltpu.SemaphoreType.DMA((n_sp - 1,)),
            pltpu.SemaphoreType.DMA((n_tp - 1,)),
            pltpu.SemaphoreType.DMA((n_tp - 1,)),
        ],
        compiler_params=pltpu.CompilerParams(collective_id=1, has_side_effects=True),
    )(ada_rows, *weights)
    tp = lax.axis_index("tp")
    order = lax.rem(tp + n_tp - jnp.arange(n_tp), n_tp)
    got = jnp.take(got, order, axis=0)
    return got.transpose(1, 0, 2).reshape(3, 8, n_tp * cols)


def gather_kernel(latent_ref, ctx_ref, ext_ref, all_ref, own_sem, s_ext, r_ext, s_ctx, r_ctx):
    sp, tp = lax.axis_index("sp"), lax.axis_index("tp")
    n_sp = lax.axis_size("sp")
    y, c = tp // 2, lax.rem(tp, 2)
    sib, across = y * 2 + 1 - c, (1 - y) * 2 + c
    always = sp >= 0
    has_up, has_down = sp > 0, sp < n_sp - 1
    direct = y * c + (1 - y) * (6 + c)
    indirect = (1 - y) * c + y * (6 + c)
    has_direct = ((y == 1) & has_up) | ((y == 0) & has_down)
    has_indirect = ((y == 0) & has_up) | ((y == 1) & has_down)
    toward = sp + 2 * y - 1
    away = sp - 2 * y + 1
    here, there = (sp, sib), (sp, across)
    own_slot, across_slot = 2 + tp, 2 + across
    x_peer = sp + 1 - 2 * lax.rem(sp, 2)
    entry_barrier(
        [
            (here, always),
            (there, always),
            ((x_peer, tp), always),
            ((sp + 2, tp), sp + 2 < n_sp),
            ((sp - 2, tp), sp >= 2),
            ((sp + 1, tp), has_down & (lax.rem(sp, 2) == 1)),
            ((sp - 1, tp), has_up & (lax.rem(sp, 2) == 0)),
        ]
    )

    def piece(flow, s, device, slot, own=False, at=None):
        return pltpu.make_async_remote_copy(
            src_ref=latent_ref.at[s] if own else ext_ref.at[s, slot if at is None else at],
            dst_ref=ext_ref.at[s, slot],
            send_sem=s_ext.at[flow, s],
            recv_sem=r_ext.at[flow, s],
            device_id=device,
            device_id_type=MESH,
        )

    sends = []

    def send(cond, copy):
        sends.append((cond, copy))

        @pl.when(cond)
        def _():
            copy.start()

    def arrived(cond, copy):
        @pl.when(cond)
        def _():
            copy.wait_recv()

    blocks = {}

    def block(at, way, device, own=False):
        return pltpu.make_async_remote_copy(
            src_ref=ctx_ref if own else all_ref.at[at],
            dst_ref=all_ref.at[at],
            send_sem=s_ctx.at[at, way],
            recv_sem=r_ctx.at[at],
            device_id=device,
            device_id_type=MESH,
        )

    up, down = (sp + 2, tp), (sp - 2, tp)
    can_up, can_down = sp + 2 < n_sp, sp >= 2
    mine = [pltpu.make_async_copy(latent_ref.at[s], ext_ref.at[s, own_slot], own_sem.at[s]) for s in range(2)]
    mine.append(pltpu.make_async_copy(ctx_ref, all_ref.at[sp], own_sem.at[2]))
    send(always, block(sp, 0, (x_peer, tp), True))
    send(can_up, block(sp, 1, up, True))
    send(can_down, block(sp, 2, down, True))
    for s in range(2):
        send(always, piece(1, s, there, own_slot, True))
        send(has_indirect, piece(2, s, (toward, tp), direct, True))
    for s in range(2):
        send(always, piece(0, s, here, own_slot, True))
    for copy in mine:
        copy.start()
    arrived(always, block(x_peer, 0, (x_peer, tp)))
    send(can_up, block(x_peer, 1, up))
    send(can_down, block(x_peer, 2, down))

    def relay(hop):
        for e in range(2):
            at = sp - lax.rem(sp, 2) - 2 * hop + e
            arrived(at >= 0, block(lax.max(at, 0), 1, up))
            send((at >= 0) & can_up, block(lax.max(at, 0), 1, up))
            low = sp - lax.rem(sp, 2) + 2 * hop + e
            arrived(low < n_sp, block(lax.min(low, n_sp - 1), 2, down))
            send((low < n_sp) & can_down, block(lax.min(low, n_sp - 1), 2, down))

    arrived(always, piece(1, 0, there, across_slot))
    send(always, piece(3, 0, here, across_slot))
    arrived(has_direct, piece(2, 0, here, direct))
    send(has_direct, piece(5, 0, there, direct))
    send(has_direct, piece(6, 0, here, direct))
    relay(1)
    arrived(always, piece(1, 1, there, across_slot))
    send(has_direct, piece(4, 1, (away, tp), indirect, at=across_slot))
    send(always, piece(3, 1, here, across_slot))
    arrived(has_direct, piece(2, 1, here, direct))
    send(has_direct, piece(6, 1, here, direct))
    for hop in range(2, n_sp // 2):
        relay(hop)
    arrived(has_indirect, piece(5, 0, there, indirect))
    send(has_indirect, piece(7, 0, here, indirect))
    arrived(has_indirect, piece(4, 1, there, indirect))
    send(has_indirect, piece(7, 1, here, indirect))
    for s in range(2):
        arrived(always, piece(0, s, here, own_slot))
        arrived(always, piece(3, s, here, own_slot))
        arrived(has_direct, piece(6, s, here, direct))
        arrived(has_indirect, piece(7, s, here, indirect))
    for cond, copy in sends:
        @pl.when(cond)
        def _():
            copy.wait_send()
    for copy in mine:
        copy.wait()


def gather_tokens(latent, ctx_pair):
    n_sp = lax.axis_size("sp")
    samples, tokens, width = latent.shape
    return pl.pallas_call(
        gather_kernel,
        out_shape=(
            jax.ShapeDtypeStruct((samples, 8, tokens, width), latent.dtype),
            jax.ShapeDtypeStruct((n_sp,) + ctx_pair.shape, ctx_pair.dtype),
        ),
        in_specs=[pl.BlockSpec(memory_space=pl.ANY)] * 2,
        out_specs=[pl.BlockSpec(memory_space=pl.ANY)] * 2,
        scratch_shapes=[
            pltpu.SemaphoreType.DMA((3,)),
            pltpu.SemaphoreType.DMA((8, 2)),
            pltpu.SemaphoreType.DMA((8, 2)),
            pltpu.SemaphoreType.DMA((n_sp, 3)),
            pltpu.SemaphoreType.DMA((n_sp,)),
        ],
        compiler_params=pltpu.CompilerParams(collective_id=2, has_side_effects=True),
    )(latent, ctx_pair)


def scatter_kernel(parts_ref, out_ref, got, summed, far, s1, r1, s2, r2):
    sp, tp = lax.axis_index("sp"), lax.axis_index("tp")
    y, c = tp // 2, lax.rem(tp, 2)
    sib, across = y * 2 + 1 - c, (1 - y) * 2 + c
    sib_across = (1 - y) * 2 + 1 - c
    entry_barrier([((sp, sib), sp >= 0), ((sp, across), sp >= 0)])
    chunks = far.shape[0]
    rows = far.shape[1]

    def near(k):
        at = k % chunks
        target = sib_across if k < chunks else sib
        return pltpu.make_async_remote_copy(
            src_ref=parts_ref.at[target, pl.ds(at * rows, rows)],
            dst_ref=got.at[k],
            send_sem=s1.at[k], recv_sem=r1.at[k],
            device_id=(sp, sib), device_id_type=MESH,
        )

    def cross(k):
        return pltpu.make_async_remote_copy(
            src_ref=summed.at[k],
            dst_ref=far.at[k],
            send_sem=s2.at[k], recv_sem=r2.at[k],
            device_id=(sp, across), device_id_type=MESH,
        )

    for k in range(2 * chunks):
        near(k).start()
    for k in range(chunks):
        near(k).wait()
        mine = parts_ref[across, k * rows : (k + 1) * rows, :].astype(jnp.float32)
        summed[k] = (mine + got[k].astype(jnp.float32)).astype(jnp.bfloat16)
        cross(k).start()
    for k in range(chunks):
        near(chunks + k).wait()
        cross(k).wait()
        mine = parts_ref[tp, k * rows : (k + 1) * rows, :].astype(jnp.float32)
        mine = mine + got[chunks + k].astype(jnp.float32) + far[k].astype(jnp.float32)
        out_ref[k * rows : (k + 1) * rows, :] = mine


def scatter_sum(parts):
    _, tokens, width = parts.shape
    chunks = 4
    rows = tokens // chunks
    sems = [pltpu.SemaphoreType.DMA((2 * chunks,))] * 2 + [pltpu.SemaphoreType.DMA((chunks,))] * 2
    return pl.pallas_call(
        scatter_kernel,
        out_shape=jax.ShapeDtypeStruct((tokens, width), jnp.float32),
        in_specs=[pl.BlockSpec(memory_space=pltpu.VMEM)],
        out_specs=pl.BlockSpec(memory_space=pltpu.VMEM),
        scratch_shapes=[
            pltpu.VMEM((2 * chunks, rows, width), jnp.bfloat16),
            pltpu.VMEM((chunks, rows, width), jnp.bfloat16),
            pltpu.VMEM((chunks, rows, width), jnp.bfloat16),
        ]
        + sems,
        compiler_params=pltpu.CompilerParams(
            collective_id=3, has_side_effects=True, vmem_limit_bytes=40 * 2**20
        ),
    )(parts)


def on_four(
    latent, context, cond, ctx_cond, w_shift, w_scale, w_gate, norm_gain,
    w_query, w_key, w_value, w_out, rel_bias, ctx_bias,
):
    samples, tokens, width = latent.shape
    n_sp, n_tp = lax.axis_size("sp"), lax.axis_size("tp")
    rows_sp, local_cols = w_shift.shape
    sp = lax.axis_index("sp")
    ada = silu_rows(jnp.concatenate([cond, ctx_cond[None, :]], axis=0))
    ada_rows = lax.dynamic_slice_in_dim(ada, sp * rows_sp, rows_sp, 1)
    modulation = modulation_vectors(ada_rows, (w_shift, w_scale, w_gate))
    ctx_hidden = modulate_rows(context, norm_gain, modulation[0, samples], modulation[1, samples])
    w_pair = jnp.concatenate([w_key, w_value], axis=1)
    own_pair = jnp.dot(ctx_hidden, w_pair, preferred_element_type=jnp.float32).astype(jnp.bfloat16)
    ext, ctx_all = gather_tokens(latent, own_pair)
    ctx_pair = ctx_all.transpose(1, 0, 2, 3).reshape(samples, -1, 2 * local_cols)
    hidden = modulate_rows(
        ext, norm_gain, modulation[0, :samples, None, None, :], modulation[1, :samples, None, None, :]
    )
    slot = jnp.arange(8)[None, :, None, None]
    valid = ((slot >= 2) | (sp > 0)) & ((slot < 6) | (sp < n_sp - 1))
    hidden = jnp.where(valid, hidden, jnp.zeros_like(hidden))
    rows_dev = n_tp * tokens // GRID_W
    pair = jnp.dot(hidden, w_pair, preferred_element_type=jnp.float32).astype(jnp.bfloat16)
    pair = pair.reshape(samples, 2 * rows_dev, GRID_W, 2 * local_cols)
    query = jnp.dot(hidden[:, 2:6], w_query, preferred_element_type=jnp.float32)
    query = query.astype(jnp.bfloat16).reshape(samples, rows_dev, GRID_W, local_cols)
    half = WIN_COLS // 2
    rolled = jnp.roll(query, half, axis=2)
    mixed = attention(rolled, pair, ctx_pair, rel_bias, ctx_bias)
    attended = jnp.roll(mixed, -half, axis=2).reshape(samples, n_tp, tokens, local_cols)
    attended = attended.transpose(1, 0, 2, 3).reshape(n_tp, samples * tokens, local_cols)
    parts = jnp.dot(attended, w_out, preferred_element_type=jnp.float32).astype(jnp.bfloat16)
    update = scatter_sum(parts).reshape(samples, tokens, width)
    gate = modulation[2, :samples, None, :]
    return (latent.astype(jnp.float32) + gate * update).astype(jnp.bfloat16)


def solution(mesh):
    shape = dict(mesh.shape)
    quick = shape["tp"] == 4 and shape["sp"] % 2 == 0
    return jax.shard_map(
        on_four if quick else on_device,
        mesh=mesh,
        in_specs=(
            P(None, ("sp", "tp"), None),
            P(None, "sp", None),
            P(),
            P(),
            P("sp", "tp"),
            P("sp", "tp"),
            P("sp", "tp"),
            P(),
            P(None, "tp"),
            P(None, "tp"),
            P(None, "tp"),
            P("tp", None),
            P("tp", None, None),
            P("tp"),
        ),
        out_specs=P(None, ("sp", "tp"), None),
        check_vma=False,
    )
```

```python
import functools

import jax
import jax.numpy as jnp
from jax import lax
from jax.experimental import pallas as pl
from jax.experimental.pallas import tpu as pltpu
from jax.sharding import PartitionSpec as P

HEAD_DIM = 64
GRID_W = 64
WIN_ROWS = 8
WIN_COLS = 16


EPSILON = 1e-06


def extended(shard, sides, width):
    for axis, dim in sides:
        size, length = (lax.axis_size(axis), shard.shape[dim])
        up = [(i, (i + 1) % size) for i in range(size - 1)]
        down = [(j, i) for i, j in up]
        last = lax.slice_in_dim(shard, length - width, length, axis=dim)
        first = lax.slice_in_dim(shard, 0, width, axis=dim)
        before = lax.ppermute(last, axis, up)
        after = lax.ppermute(first, axis, down)
        shard = jnp.concatenate([before, shard, after], axis=dim)
    return shard


def silu_rows(values):
    return jax.nn.silu(values.astype(jnp.float32)).astype(jnp.bfloat16)


def modulate_rows(rows, gain, shift, scale):
    floats = rows.astype(jnp.float32)
    inverse = lax.rsqrt(jnp.mean(floats * floats, axis=-1, keepdims=True) + EPSILON)
    return (floats * inverse * gain * (1.0 + scale) + shift).astype(jnp.bfloat16)

LOG2E = 1.4426950408889634


def attention_kernel(bias_ref, far_ref, q_ref, k_ref, v_ref, ck_ref, cv_ref, out_ref, table):
    pair = pl.program_id(0)
    rows_dev = q_ref.shape[1]
    padded = k_ref.shape[1]
    span = 2 * WIN_COLS
    half = WIN_COLS // 2
    reach = WIN_ROWS // 2
    nq, nk = rows_dev * WIN_COLS, padded * span
    lanes = 2 * HEAD_DIM

    @pl.when(pl.program_id(1) == 0)
    def _():
        sp = lax.axis_index("sp")
        rows_all = rows_dev * lax.axis_size("sp")
        at = lax.broadcasted_iota(jnp.int32, (WIN_COLS, nk), 1)
        p = lax.broadcasted_iota(jnp.int32, (WIN_COLS, nk), 0)
        key_row = sp * rows_dev - reach + at // span
        k = at % span
        inner = (k - p >= 0) & (k - p < WIN_COLS)
        edge = (p < half) == (k < WIN_COLS)
        for r in range(rows_dev):
            row = sp * rows_dev + r
            first = jnp.clip(row - reach, 0, rows_all - WIN_ROWS)
            inside = (key_row >= first) & (key_row < first + WIN_ROWS)
            shift = span * (r + reach - WIN_ROWS + 1) - half + 1
            for h in range(2):
                line = jnp.broadcast_to(bias_ref[0, h : h + 1, :], (WIN_COLS, nk))
                line = pltpu.roll(line, shift % nk, 1, stride=1, stride_axis=0) * LOG2E
                at_rows = pl.ds(r * WIN_COLS, WIN_COLS)
                table[h, 0, at_rows, :] = jnp.where(inside & edge, line, -jnp.inf)
                table[h, 1, at_rows, :] = jnp.where(inside & inner, line, -jnp.inf)

    factor = HEAD_DIM ** (-0.5) * LOG2E
    ck = ck_ref[...].reshape(-1, lanes)
    ctx_count = ck.shape[0]
    cv = jnp.concatenate([cv_ref[...].reshape(-1, lanes), jnp.ones((ctx_count, lanes), jnp.bfloat16)], axis=1)
    ones = jnp.ones((nk, lanes), jnp.bfloat16)
    low = lax.broadcasted_iota(jnp.int32, (nq, lanes), 1) < HEAD_DIM
    contract = (((1,), (1,)), ((), ()))
    for block in range(GRID_W // WIN_COLS):
        q = q_ref[0, :, WIN_COLS * block : WIN_COLS * (block + 1), :].reshape(nq, lanes)

        def keys(ref):
            if block == 0:
                got = jnp.concatenate([ref[0, :, GRID_W - WIN_COLS :, :], ref[0, :, :WIN_COLS, :]], 1)
            else:
                got = ref[0, :, WIN_COLS * (block - 1) : WIN_COLS * (block + 1), :]
            return got.reshape(nk, lanes)

        k = keys(k_ref)
        v = jnp.concatenate([keys(v_ref), ones], axis=1)
        halves = []
        for h in range(2):
            mine = low if h == 0 else jnp.logical_not(low)
            one = jnp.where(mine, q, jnp.zeros_like(q))
            near = lax.dot_general(one, k, contract, preferred_element_type=jnp.float32)
            near = near * factor + table[h, min(block, 1)]
            far = lax.dot_general(one, ck, contract, preferred_element_type=jnp.float32)
            far = far * factor + far_ref[2 * pair + h] * LOG2E
            top = jnp.maximum(
                jnp.max(near, axis=-1, keepdims=True), jnp.max(far, axis=-1, keepdims=True)
            )
            near = jnp.exp2(near - top).astype(jnp.bfloat16)
            far = jnp.exp2(far - top).astype(jnp.bfloat16)
            got = jnp.dot(near, v, preferred_element_type=jnp.float32) + jnp.dot(
                far, cv, preferred_element_type=jnp.float32
            )
            halves.append(got[:, :lanes] / got[:, lanes:])
        got = jnp.where(low, halves[0], halves[1]).astype(jnp.bfloat16)
        out_ref[0, :, WIN_COLS * block : WIN_COLS * (block + 1), :] = got.reshape(
            rows_dev, WIN_COLS, lanes
        )


def attention(query, pair, ctx_pair, rel_bias, ctx_bias):
    samples, rows_dev, _, cols = query.shape
    padded, ctx_count = pair.shape[1], ctx_pair.shape[0] * ctx_pair.shape[2]
    heads = cols // HEAD_DIM
    lanes = 2 * HEAD_DIM
    pairs = cols // lanes
    nq, nk = rows_dev * WIN_COLS, padded * 2 * WIN_COLS
    flat = jnp.pad(rel_bias, ((0, 0), (0, 1), (0, 1))).reshape(heads, -1)
    flat = jnp.pad(flat, ((0, 0), (0, nk - flat.shape[1]))).reshape(pairs, 2, nk)
    token = lambda at: pl.BlockSpec((1, padded, GRID_W, lanes), lambda p, s: (s, 0, 0, p + at))
    far = lambda at: pl.BlockSpec(
        (ctx_pair.shape[0], 1, ctx_pair.shape[2], lanes), lambda p, s: (0, s, 0, p + at)
    )
    own = pl.BlockSpec((1, rows_dev, GRID_W, lanes), lambda p, s: (s, 0, 0, p))
    scores = samples * heads * 4 * nq * (nk + ctx_count)
    return pl.pallas_call(
        attention_kernel,
        grid=(pairs, samples),
        out_shape=jax.ShapeDtypeStruct(query.shape, jnp.bfloat16),
        in_specs=[
            pl.BlockSpec((1, 2, nk), lambda p, s: (p, 0, 0)),
            pl.BlockSpec(memory_space=pltpu.SMEM),
            own,
            token(0),
            token(pairs),
            far(0),
            far(pairs),
        ],
        out_specs=own,
        scratch_shapes=[pltpu.VMEM((2, 2, nq, nk), jnp.float32)],
        cost_estimate=pl.CostEstimate(
            flops=scores * 512, bytes_accessed=8 * query.size * 2, transcendentals=scores
        ),
    )(flat, ctx_bias, query, pair, pair, ctx_pair, ctx_pair)


def on_device(
    latent,
    context,
    cond,
    ctx_cond,
    w_shift,
    w_scale,
    w_gate,
    norm_gain,
    w_query,
    w_key,
    w_value,
    w_out,
    rel_bias,
    ctx_bias,
):
    samples = latent.shape[0]
    rows_sp = w_shift.shape[0]
    local_cols = w_shift.shape[1]
    sp_index = lax.axis_index("sp")
    ada = silu_rows(jnp.concatenate([cond, ctx_cond[None, :]], axis=0))
    ada_rows = lax.dynamic_slice_in_dim(ada, sp_index * rows_sp, rows_sp, 1)
    partial_value = jnp.stack(
        [
            jnp.dot(ada_rows, weight, preferred_element_type=jnp.float32)
            for weight in (w_shift, w_scale, w_gate)
        ]
    )
    summed = lax.psum(partial_value, "sp")
    modulation = lax.all_gather(summed, "tp", axis=2, tiled=True)
    hidden = modulate_rows(
        latent, norm_gain, modulation[0, :samples, None, :], modulation[1, :samples, None, :]
    )
    w_triple = jnp.concatenate([w_query, w_key, w_value], axis=1)
    triple = jnp.dot(
        lax.all_gather(hidden, "tp", axis=1, tiled=True),
        w_triple,
        preferred_element_type=jnp.float32,
    ).astype(jnp.bfloat16)
    ctx_hidden = modulate_rows(context, norm_gain, modulation[0, samples], modulation[1, samples])
    w_pair = jnp.concatenate([w_key, w_value], axis=1)
    own_pair = jnp.dot(ctx_hidden, w_pair, preferred_element_type=jnp.float32).astype(jnp.bfloat16)
    ctx_pair = lax.all_gather(own_pair, "sp", axis=1, tiled=True)
    heads = local_cols // HEAD_DIM
    tokens_sp = triple.shape[1]
    rows_dev = tokens_sp // GRID_W
    rows_all = rows_dev * lax.axis_size("sp")
    reach = WIN_ROWS // 2
    query = triple[..., :local_cols].reshape(samples, rows_dev, GRID_W, local_cols)
    pair = triple[..., local_cols:].reshape(samples, rows_dev, GRID_W, 2 * local_cols)
    padded_pair = extended(pair, (("sp", 1),), reach)
    half = WIN_COLS // 2
    rolled = jnp.roll(query, half, axis=2)
    mixed = attention(rolled, padded_pair, ctx_pair[None], rel_bias, ctx_bias)
    attended = jnp.roll(mixed, -half, axis=2).reshape(samples, tokens_sp, local_cols)
    attended = attended.transpose(1, 0, 2)
    update = lax.psum_scatter(
        jnp.einsum("tsc,cd->tsd", attended, w_out, preferred_element_type=jnp.float32).astype(
            jnp.bfloat16
        ),
        "tp",
        scatter_dimension=0,
        tiled=True,
    ).astype(jnp.float32)
    gate = modulation[2, :samples, None, :]
    result = latent.astype(jnp.float32) + gate * update.transpose(1, 0, 2)
    return result.astype(jnp.bfloat16)


MESH = pl.DeviceIdType.MESH


def entry_barrier(peers):
    barrier = pltpu.get_barrier_semaphore()
    for device, there in peers:
        @pl.when(there)
        def _():
            pl.semaphore_signal(barrier, inc=1, device_id=device, device_id_type=MESH)
    pl.semaphore_wait(barrier, sum(jnp.where(there, 1, 0) for _, there in peers))


def front_kernel(
    ada_ref, ws_ref, wc_ref, wg_ref, gain_ref, latent_ref, ctx_ref, wq_ref, wk_ref, wv_ref,
    full_ref, q_ref, kv_ref, ckv_ref,
    part, got, total, full, buf, wq, wkv, own_sem, s1, r1, s2, r2, s_ext, r_ext, s_ctx, r_ctx, r_sib,
):
    sp, tp = lax.axis_index("sp"), lax.axis_index("tp")
    n_sp, n_tp = lax.axis_size("sp"), lax.axis_size("tp")
    cols = part.shape[1]
    over_sp = [lax.rem(sp + k, n_sp) for k in range(1, n_sp)]
    over_tp = [lax.rem(tp + k, n_tp) for k in range(1, n_tp)]
    always = sp >= 0
    y, c = tp // 2, lax.rem(tp, 2)
    z, x = sp // 2, lax.rem(sp, 2)
    n_z = n_sp // 2
    sib, across = y * 2 + 1 - c, (1 - y) * 2 + c
    has_up, has_down = sp > 0, sp < n_sp - 1
    direct = y * c + (1 - y) * (6 + c)
    indirect = (1 - y) * c + y * (6 + c)
    has_direct = ((y == 1) & has_up) | ((y == 0) & has_down)
    has_indirect = ((y == 0) & has_up) | ((y == 1) & has_down)
    toward = sp + 2 * y - 1
    here, there = (sp, sib), (sp, across)
    own_slot, across_slot = 2 + tp, 2 + across
    x_peer = sp + 1 - 2 * x
    beside, up, down = (x_peer, tp), (sp + 2, tp), (sp - 2, tp)
    can_up, can_down = sp + 2 < n_sp, sp >= 2
    half = buf.shape[1] // 2
    part_of = pl.ds(pl.multiple_of(c * half, half), half)

    locals_ = [
        pltpu.make_async_copy(wq_ref, wq, own_sem.at[0]),
        pltpu.make_async_copy(wk_ref, wkv.at[:, pl.ds(0, cols)], own_sem.at[1]),
        pltpu.make_async_copy(wv_ref, wkv.at[:, pl.ds(cols, cols)], own_sem.at[2]),
    ]
    for copy in locals_:
        copy.start()
    own_copies = [
        pltpu.make_async_copy(latent_ref.at[s], buf.at[s * 8 + own_slot], own_sem.at[3 + s])
        for s in range(2)
    ] + [
        pltpu.make_async_copy(ctx_ref.at[s], buf.at[16 + sp, pl.ds(half * s, half)], own_sem.at[5 + s])
        for s in range(2)
    ]
    for copy in own_copies:
        copy.start()
    entry_barrier([((p, tp), always) for p in over_sp] + [((sp, p), always) for p in over_tp])

    early = []
    mode = ["start"]

    def send(cond, copy):
        @pl.when(cond)
        def _():
            if mode[0] == "start":
                copy.start()
            else:
                copy.wait_send()

    def begin(cond, copy):
        early.append((cond, copy))
        send(cond, copy)

    def arrived(cond, copy):
        if mode[0] == "start":
            @pl.when(cond)
            def _():
                copy.wait_recv()

    def piece(flow, s, device, slot, own=False):
        return pltpu.make_async_remote_copy(
            src_ref=latent_ref.at[s] if own else buf.at[s * 8 + slot],
            dst_ref=buf.at[s * 8 + slot],
            send_sem=s_ext.at[flow, s], recv_sem=r_ext.at[flow, s],
            device_id=device, device_id_type=MESH,
        )

    def block(at, way, device, own=False):
        return pltpu.make_async_remote_copy(
            src_ref=ctx_ref.at[c] if own else buf.at[16 + at, part_of],
            dst_ref=buf.at[16 + at, part_of],
            send_sem=s_ctx.at[at, way], recv_sem=(r_sib if way == 3 else r_ctx).at[at],
            device_id=device, device_id_type=MESH,
        )

    def first(k, peer):
        return pltpu.make_async_remote_copy(
            src_ref=part, dst_ref=got.at[k], send_sem=s1.at[k], recv_sem=r1.at[k],
            device_id=(peer, tp), device_id_type=MESH,
        )

    columns = pl.ds(pl.multiple_of(tp * cols, cols), cols)

    def second(k, peer):
        return pltpu.make_async_remote_copy(
            src_ref=total, dst_ref=full.at[:, columns], send_sem=s2.at[k], recv_sem=r2.at[k],
            device_id=(sp, peer), device_id_type=MESH,
        )

    for at, weight in enumerate((ws_ref, wc_ref, wg_ref)):
        value = jnp.dot(ada_ref[...], weight[...], preferred_element_type=jnp.float32)
        part[8 * at : 8 * at + 8, :] = value[:8]
    firsts = [first(k, peer) for k, peer in enumerate(over_sp)]
    for copy in firsts:
        copy.start()
    begin(always, piece(1, 0, there, own_slot, True))
    begin(always, block(sp, 0, beside, True))
    begin(can_up, block(sp, 1, up, True))
    begin(can_down, block(sp, 2, down, True))
    for s in range(2):
        begin(has_indirect, piece(2, s, (toward, tp), direct, True))
    for s in range(2):
        begin(always, piece(0, s, here, own_slot, True))
    value = part[...]
    for k, copy in enumerate(firsts):
        copy.wait()
        value = value + got[k]
    total[...] = value
    seconds = [second(k, peer) for k, peer in enumerate(over_tp)]
    for copy in seconds:
        copy.start()
    begin(always, piece(1, 1, there, own_slot, True))
    full[:, columns] = value
    for copy in locals_ + own_copies:
        copy.wait()
    for copy in seconds:
        copy.wait()
    full_ref[...] = full[...]

    def neighbour_block():
        arrived(always, block(x_peer, 0, beside))
        send((c == 0) & can_up, block(x_peer, 1, up))
        send((c == 0) & can_down, block(x_peer, 2, down))
        send(always, block(x_peer, 3, here))

    def relay(hop):
        for e in range(2):
            straight = (c == 0) | (x == e)
            crossing = (c == 1) & (x == e)
            low, high = sp - x - 2 * hop + e, sp - x + 2 * hop + e
            for at, way, device, can, there_is in (
                (lax.max(low, 0), 1, up, can_up, low >= 0),
                (lax.min(high, n_sp - 1), 2, down, can_down, high < n_sp),
            ):
                arrived(there_is, block(at, way, device))
                send(there_is & can & straight, block(at, way, device))
                send(there_is & crossing, block(at, 0, beside))
                send(there_is, block(at, 3, here))

    def from_across(s):
        arrived(always, piece(1, s, there, across_slot))
        send(always, piece(3, s, here, across_slot))

    def from_direct(s):
        arrived(has_direct, piece(2, s, here, direct))
        send(has_direct, piece(5, s, there, direct))
        send(has_direct, piece(6, s, here, direct))

    def from_indirect(s):
        arrived(has_indirect, piece(5, s, there, indirect))
        send(has_indirect, piece(7, s, here, indirect))

    def sibling(flow, s, cond=always):
        arrived(cond, piece(flow, s, here, own_slot))

    def far_block(h, e):
        zb = lax.rem(z + h, n_z)
        at = 2 * zb + e
        arrived(always, block(at, 3, here))

    plan = []

    def add(kind, s, events, at=0):
        plan.append((kind, s, events, at))

    add(0, 0, [])
    add(0, 1, [])
    add(1, 0, [neighbour_block, lambda: sibling(0, 0)])
    add(1, 1, [lambda: sibling(0, 1)])
    add(8, 0, [lambda: from_across(0)], sp)
    add(2, 0, [lambda: from_direct(0)])
    add(4, 0, [lambda: relay(1)] if n_z > 1 else [])
    add(3, 0, [lambda: sibling(3, 0)])
    add(5, 0, [lambda: sibling(6, 0, has_direct)])
    add(8, 0, [lambda: arrived(always, block(x_peer, 3, here))], x_peer)
    add(2, 1, [lambda: from_across(1)] + ([lambda: relay(2)] if n_z > 2 else []))
    add(4, 1, [lambda: from_direct(1)])
    add(3, 1, [lambda: sibling(3, 1)])
    add(5, 1, [lambda: sibling(6, 1, has_direct)])
    add(6, 0, [lambda: from_indirect(0)])
    for hop in range(3, n_z):
        plan[-1][2].append(functools.partial(relay, hop))
    add(7, 0, [lambda: sibling(7, 0, has_indirect)])
    for h in range(1, n_z):
        for e in range(2):
            add(8, 0, [functools.partial(far_block, h, e)], 2 * lax.rem(z + h, n_z) + e)
    add(6, 1, [lambda: from_indirect(1)])
    add(7, 1, [lambda: sibling(7, 1, has_indirect)])

    slots = (own_slot, 2 + sib, across_slot, 2 + (1 - y) * 2 + 1 - c,
             direct, direct + 1 - 2 * c, indirect, indirect + 1 - 2 * c)

    def step(i, carry):
        at = 0
        row = 0
        exists = 0
        wants = 0
        for k, (kind, s, events, ctx_at) in enumerate(plan):
            on = jnp.where(i == k, 1, 0)
            at = at + on * (16 + ctx_at if kind == 8 else s * 8 + slots[kind])
            row = row + on * (2 if kind == 8 else s)
            there_is = has_direct if kind in (4, 5) else has_indirect if kind in (6, 7) else always
            exists = exists + on * jnp.where(there_is, 1, 0)
            wants = wants + on * (1 if kind < 4 else 0)
            if events:
                @pl.when(i == k)
                def _():
                    for event in events:
                        event()

        @pl.when(exists == 1)
        def _():
            rows = buf[at].astype(jnp.float32)
            inverse = lax.rsqrt(jnp.mean(rows * rows, axis=-1, keepdims=True) + EPSILON)
            lift = gain_ref[...] * (1.0 + full[pl.ds(8 + row, 1), :])
            hidden = (rows * inverse * lift + full[pl.ds(row, 1), :]).astype(jnp.bfloat16)
            pair = jnp.dot(hidden, wkv[...], preferred_element_type=jnp.float32).astype(jnp.bfloat16)

            @pl.when(at < 16)
            def _():
                kv_ref[lax.min(at, 15)] = pair

            @pl.when(at >= 16)
            def _():
                ckv_ref[lax.max(at - 16, 0)] = pair

            @pl.when(wants == 1)
            def _():
                place = lax.min(lax.max(at - 2 - 4 * row, 0), 7)
                q_ref[place] = jnp.dot(
                    hidden, wq[...], preferred_element_type=jnp.float32
                ).astype(jnp.bfloat16)

        @pl.when(exists == 0)
        def _():
            kv_ref[lax.min(at, 15)] = jnp.zeros(kv_ref.shape[1:], jnp.bfloat16)

        return carry

    lax.fori_loop(0, len(plan), step, 0)
    mode[0] = "drain"
    for cond, copy in early:
        send(cond, copy)
    for _, _, events, _ in plan:
        for event in events:
            event()


def front(ada_rows, mods, gain, latent, context, w_query, w_key, w_value):
    n_sp, n_tp = lax.axis_size("sp"), lax.axis_size("tp")
    samples, tokens, width = latent.shape
    cols = w_query.shape[1]
    block = (24, cols)
    ada_rows = jnp.pad(ada_rows, ((0, 16 - ada_rows.shape[0]), (0, 0)))
    vmem, hbm = pl.BlockSpec(memory_space=pltpu.VMEM), pl.BlockSpec(memory_space=pl.ANY)
    dma = pltpu.SemaphoreType.DMA
    return pl.pallas_call(
        front_kernel,
        out_shape=(
            jax.ShapeDtypeStruct((24, width), jnp.float32),
            jax.ShapeDtypeStruct((samples * n_tp, tokens, cols), jnp.bfloat16),
            jax.ShapeDtypeStruct((samples * 8, tokens, 2 * cols), jnp.bfloat16),
            jax.ShapeDtypeStruct((n_sp, samples * context.shape[1], 2 * cols), jnp.bfloat16),
        ),
        in_specs=[vmem] * 7 + [hbm] * 3,
        out_specs=[vmem] * 4,
        scratch_shapes=[
            pltpu.VMEM(block, jnp.float32),
            pltpu.VMEM((n_sp - 1,) + block, jnp.float32),
            pltpu.VMEM(block, jnp.float32),
            pltpu.VMEM((24, width), jnp.float32),
            pltpu.VMEM((16 + n_sp, tokens, width), jnp.bfloat16),
            pltpu.VMEM((width, cols), jnp.bfloat16),
            pltpu.VMEM((width, 2 * cols), jnp.bfloat16),
            dma((7,)), dma((n_sp - 1,)), dma((n_sp - 1,)), dma((n_tp - 1,)), dma((n_tp - 1,)),
            dma((8, 2)), dma((8, 2)), dma((n_sp, 4)), dma((n_sp,)), dma((n_sp,)),
        ],
        compiler_params=pltpu.CompilerParams(
            collective_id=1, has_side_effects=True, vmem_limit_bytes=60 * 2**20
        ),
    )(ada_rows, *mods, gain[None, :], latent, context, w_query, w_key, w_value)


def scatter_kernel(parts_ref, out_ref, got, summed, far, s1, r1, s2, r2):
    sp, tp = lax.axis_index("sp"), lax.axis_index("tp")
    y, c = tp // 2, lax.rem(tp, 2)
    sib, across = y * 2 + 1 - c, (1 - y) * 2 + c
    sib_across = (1 - y) * 2 + 1 - c
    entry_barrier([((sp, sib), sp >= 0), ((sp, across), sp >= 0)])
    chunks = far.shape[0]
    rows = far.shape[1]

    def near(k):
        at = k % chunks
        target = sib_across if k < chunks else sib
        return pltpu.make_async_remote_copy(
            src_ref=parts_ref.at[target, pl.ds(at * rows, rows)],
            dst_ref=got.at[k],
            send_sem=s1.at[k], recv_sem=r1.at[k],
            device_id=(sp, sib), device_id_type=MESH,
        )

    def cross(k):
        return pltpu.make_async_remote_copy(
            src_ref=summed.at[k],
            dst_ref=far.at[k],
            send_sem=s2.at[k], recv_sem=r2.at[k],
            device_id=(sp, across), device_id_type=MESH,
        )

    for k in range(2 * chunks):
        near(k).start()
    for k in range(chunks):
        near(k).wait()
        mine = parts_ref[across, k * rows : (k + 1) * rows, :].astype(jnp.float32)
        summed[k] = (mine + got[k].astype(jnp.float32)).astype(jnp.bfloat16)
        cross(k).start()
    for k in range(chunks):
        near(chunks + k).wait()
        cross(k).wait()
        mine = parts_ref[tp, k * rows : (k + 1) * rows, :].astype(jnp.float32)
        mine = mine + got[chunks + k].astype(jnp.float32) + far[k].astype(jnp.float32)
        out_ref[k * rows : (k + 1) * rows, :] = mine


def scatter_sum(parts):
    _, tokens, width = parts.shape
    chunks = 4
    rows = tokens // chunks
    sems = [pltpu.SemaphoreType.DMA((2 * chunks,))] * 2 + [pltpu.SemaphoreType.DMA((chunks,))] * 2
    return pl.pallas_call(
        scatter_kernel,
        out_shape=jax.ShapeDtypeStruct((tokens, width), jnp.float32),
        in_specs=[pl.BlockSpec(memory_space=pltpu.VMEM)],
        out_specs=pl.BlockSpec(memory_space=pltpu.VMEM),
        scratch_shapes=[
            pltpu.VMEM((2 * chunks, rows, width), jnp.bfloat16),
            pltpu.VMEM((chunks, rows, width), jnp.bfloat16),
            pltpu.VMEM((chunks, rows, width), jnp.bfloat16),
        ]
        + sems,
        compiler_params=pltpu.CompilerParams(
            collective_id=3, has_side_effects=True, vmem_limit_bytes=40 * 2**20
        ),
    )(parts)


def on_four(
    latent, context, cond, ctx_cond, w_shift, w_scale, w_gate, norm_gain,
    w_query, w_key, w_value, w_out, rel_bias, ctx_bias,
):
    samples, tokens, width = latent.shape
    n_sp, n_tp = lax.axis_size("sp"), lax.axis_size("tp")
    rows_sp, local_cols = w_shift.shape
    sp = lax.axis_index("sp")
    ada = silu_rows(jnp.concatenate([cond, ctx_cond[None, :]], axis=0))
    ada_rows = lax.dynamic_slice_in_dim(ada, sp * rows_sp, rows_sp, 1)
    modulation, query, pair, ctx_pair = front(
        ada_rows, (w_shift, w_scale, w_gate), norm_gain, latent, context, w_query, w_key, w_value
    )
    modulation = modulation.reshape(3, 8, width)
    rows_dev = n_tp * tokens // GRID_W
    query = query.reshape(samples, rows_dev, GRID_W, local_cols)
    pair = pair.reshape(samples, 2 * rows_dev, GRID_W, 2 * local_cols)
    ctx_pair = ctx_pair.reshape(n_sp, samples, -1, 2 * local_cols)
    half = WIN_COLS // 2
    rolled = jnp.roll(query, half, axis=2)
    mixed = attention(rolled, pair, ctx_pair, rel_bias, ctx_bias)
    attended = jnp.roll(mixed, -half, axis=2).reshape(samples, n_tp, tokens, local_cols)
    attended = attended.transpose(1, 0, 2, 3).reshape(n_tp, samples * tokens, local_cols)
    parts = jnp.dot(attended, w_out, preferred_element_type=jnp.float32).astype(jnp.bfloat16)
    update = scatter_sum(parts).reshape(samples, tokens, width)
    gate = modulation[2, :samples, None, :]
    return (latent.astype(jnp.float32) + gate * update).astype(jnp.bfloat16)


def solution(mesh):
    shape = dict(mesh.shape)
    quick = shape["tp"] == 4 and shape["sp"] == 8
    return jax.shard_map(
        on_four if quick else on_device,
        mesh=mesh,
        in_specs=(
            P(None, ("sp", "tp"), None),
            P(None, "sp", None),
            P(),
            P(),
            P("sp", "tp"),
            P("sp", "tp"),
            P("sp", "tp"),
            P(),
            P(None, "tp"),
            P(None, "tp"),
            P(None, "tp"),
            P("tp", None),
            P("tp", None, None),
            P("tp"),
        ),
        out_specs=P(None, ("sp", "tp"), None),
        check_vma=False,
    )
```

```python
import functools

import jax
import jax.numpy as jnp
from jax import lax
from jax.experimental import pallas as pl
from jax.experimental.pallas import tpu as pltpu
from jax.sharding import PartitionSpec as P

HEAD_DIM = 64
GRID_W = 64
WIN_ROWS = 8
WIN_COLS = 16


EPSILON = 1e-06


def extended(shard, sides, width):
    for axis, dim in sides:
        size, length = (lax.axis_size(axis), shard.shape[dim])
        up = [(i, (i + 1) % size) for i in range(size - 1)]
        down = [(j, i) for i, j in up]
        last = lax.slice_in_dim(shard, length - width, length, axis=dim)
        first = lax.slice_in_dim(shard, 0, width, axis=dim)
        before = lax.ppermute(last, axis, up)
        after = lax.ppermute(first, axis, down)
        shard = jnp.concatenate([before, shard, after], axis=dim)
    return shard


def silu_rows(values):
    return jax.nn.silu(values.astype(jnp.float32)).astype(jnp.bfloat16)


def modulate_rows(rows, gain, shift, scale):
    floats = rows.astype(jnp.float32)
    inverse = lax.rsqrt(jnp.mean(floats * floats, axis=-1, keepdims=True) + EPSILON)
    return (floats * inverse * gain * (1.0 + scale) + shift).astype(jnp.bfloat16)

LOG2E = 1.4426950408889634


def attention_kernel(bias_ref, far_ref, q_ref, k_ref, v_ref, ck_ref, cv_ref, out_ref, table):
    pair = pl.program_id(0)
    rows_dev = q_ref.shape[1]
    padded = k_ref.shape[1]
    span = 2 * WIN_COLS
    half = WIN_COLS // 2
    reach = WIN_ROWS // 2
    nq, nk = rows_dev * WIN_COLS, padded * span
    lanes = 2 * HEAD_DIM

    @pl.when(pl.program_id(1) == 0)
    def _():
        sp = lax.axis_index("sp")
        rows_all = rows_dev * lax.axis_size("sp")
        at = lax.broadcasted_iota(jnp.int32, (WIN_COLS, nk), 1)
        p = lax.broadcasted_iota(jnp.int32, (WIN_COLS, nk), 0)
        key_row = sp * rows_dev - reach + at // span
        k = at % span
        inner = (k - p >= 0) & (k - p < WIN_COLS)
        edge = (p < half) == (k < WIN_COLS)
        for r in range(rows_dev):
            row = sp * rows_dev + r
            first = jnp.clip(row - reach, 0, rows_all - WIN_ROWS)
            inside = (key_row >= first) & (key_row < first + WIN_ROWS)
            shift = span * (r + reach - WIN_ROWS + 1) - half + 1
            for h in range(2):
                line = jnp.broadcast_to(bias_ref[0, h : h + 1, :], (WIN_COLS, nk))
                line = pltpu.roll(line, shift % nk, 1, stride=1, stride_axis=0) * LOG2E
                at_rows = pl.ds(r * WIN_COLS, WIN_COLS)
                table[h, 0, at_rows, :] = jnp.where(inside & edge, line, -jnp.inf)
                table[h, 1, at_rows, :] = jnp.where(inside & inner, line, -jnp.inf)

    factor = HEAD_DIM ** (-0.5) * LOG2E
    ck = ck_ref[...].reshape(-1, lanes)
    ctx_count = ck.shape[0]
    cv = jnp.concatenate([cv_ref[...].reshape(-1, lanes), jnp.ones((ctx_count, lanes), jnp.bfloat16)], axis=1)
    ones = jnp.ones((nk, lanes), jnp.bfloat16)
    low = lax.broadcasted_iota(jnp.int32, (nq, lanes), 1) < HEAD_DIM
    contract = (((1,), (1,)), ((), ()))
    every = q_ref[0].astype(jnp.float32)
    outs = []
    for block in range(GRID_W // WIN_COLS):
        if block == 0:
            q = jnp.concatenate([every[:, GRID_W - half :], every[:, :half]], axis=1)
        else:
            q = every[:, WIN_COLS * block - half : WIN_COLS * (block + 1) - half]
        q = q.astype(jnp.bfloat16).reshape(nq, lanes)

        def keys(ref):
            if block == 0:
                got = jnp.concatenate([ref[0, :, GRID_W - WIN_COLS :, :], ref[0, :, :WIN_COLS, :]], 1)
            else:
                got = ref[0, :, WIN_COLS * (block - 1) : WIN_COLS * (block + 1), :]
            return got.reshape(nk, lanes)

        k = keys(k_ref)
        v = jnp.concatenate([keys(v_ref), ones], axis=1)
        halves = []
        for h in range(2):
            mine = low if h == 0 else jnp.logical_not(low)
            one = jnp.where(mine, q, jnp.zeros_like(q))
            near = lax.dot_general(one, k, contract, preferred_element_type=jnp.float32)
            near = near * factor + table[h, min(block, 1)]
            far = lax.dot_general(one, ck, contract, preferred_element_type=jnp.float32)
            far = far * factor + far_ref[2 * pair + h] * LOG2E
            top = jnp.maximum(
                jnp.max(near, axis=-1, keepdims=True), jnp.max(far, axis=-1, keepdims=True)
            )
            near = jnp.exp2(near - top).astype(jnp.bfloat16)
            far = jnp.exp2(far - top).astype(jnp.bfloat16)
            got = jnp.dot(near, v, preferred_element_type=jnp.float32) + jnp.dot(
                far, cv, preferred_element_type=jnp.float32
            )
            halves.append(got[:, :lanes] / got[:, lanes:])
        outs.append(jnp.where(low, halves[0], halves[1]).reshape(rows_dev, WIN_COLS, lanes))
    outs = [outs[0][:, half:]] + outs[1:] + [outs[0][:, :half]]
    out_ref[0] = jnp.concatenate(outs, axis=1).astype(jnp.bfloat16)


def attention(query, pair, ctx_pair, rel_bias, ctx_bias):
    samples, rows_dev, _, cols = query.shape
    padded, ctx_count = pair.shape[1], ctx_pair.shape[0] * ctx_pair.shape[2]
    heads = cols // HEAD_DIM
    lanes = 2 * HEAD_DIM
    pairs = cols // lanes
    nq, nk = rows_dev * WIN_COLS, padded * 2 * WIN_COLS
    flat = jnp.pad(rel_bias, ((0, 0), (0, 1), (0, 1))).reshape(heads, -1)
    flat = jnp.pad(flat, ((0, 0), (0, nk - flat.shape[1]))).reshape(pairs, 2, nk)
    token = lambda at: pl.BlockSpec((1, padded, GRID_W, lanes), lambda p, s: (s, 0, 0, p + at))
    far = lambda at: pl.BlockSpec(
        (ctx_pair.shape[0], 1, ctx_pair.shape[2], lanes), lambda p, s: (0, s, 0, p + at)
    )
    own = pl.BlockSpec((1, rows_dev, GRID_W, lanes), lambda p, s: (s, 0, 0, p))
    scores = samples * heads * 4 * nq * (nk + ctx_count)
    return pl.pallas_call(
        attention_kernel,
        grid=(pairs, samples),
        out_shape=jax.ShapeDtypeStruct(query.shape, jnp.bfloat16),
        in_specs=[
            pl.BlockSpec((1, 2, nk), lambda p, s: (p, 0, 0)),
            pl.BlockSpec(memory_space=pltpu.SMEM),
            own,
            token(0),
            token(pairs),
            far(0),
            far(pairs),
        ],
        out_specs=own,
        scratch_shapes=[pltpu.VMEM((2, 2, nq, nk), jnp.float32)],
        cost_estimate=pl.CostEstimate(
            flops=scores * 512, bytes_accessed=8 * query.size * 2, transcendentals=scores
        ),
    )(flat, ctx_bias, query, pair, pair, ctx_pair, ctx_pair)


def on_device(
    latent,
    context,
    cond,
    ctx_cond,
    w_shift,
    w_scale,
    w_gate,
    norm_gain,
    w_query,
    w_key,
    w_value,
    w_out,
    rel_bias,
    ctx_bias,
):
    samples = latent.shape[0]
    rows_sp = w_shift.shape[0]
    local_cols = w_shift.shape[1]
    sp_index = lax.axis_index("sp")
    ada = silu_rows(jnp.concatenate([cond, ctx_cond[None, :]], axis=0))
    ada_rows = lax.dynamic_slice_in_dim(ada, sp_index * rows_sp, rows_sp, 1)
    partial_value = jnp.stack(
        [
            jnp.dot(ada_rows, weight, preferred_element_type=jnp.float32)
            for weight in (w_shift, w_scale, w_gate)
        ]
    )
    summed = lax.psum(partial_value, "sp")
    modulation = lax.all_gather(summed, "tp", axis=2, tiled=True)
    hidden = modulate_rows(
        latent, norm_gain, modulation[0, :samples, None, :], modulation[1, :samples, None, :]
    )
    w_triple = jnp.concatenate([w_query, w_key, w_value], axis=1)
    triple = jnp.dot(
        lax.all_gather(hidden, "tp", axis=1, tiled=True),
        w_triple,
        preferred_element_type=jnp.float32,
    ).astype(jnp.bfloat16)
    ctx_hidden = modulate_rows(context, norm_gain, modulation[0, samples], modulation[1, samples])
    w_pair = jnp.concatenate([w_key, w_value], axis=1)
    own_pair = jnp.dot(ctx_hidden, w_pair, preferred_element_type=jnp.float32).astype(jnp.bfloat16)
    ctx_pair = lax.all_gather(own_pair, "sp", axis=1, tiled=True)
    heads = local_cols // HEAD_DIM
    tokens_sp = triple.shape[1]
    rows_dev = tokens_sp // GRID_W
    rows_all = rows_dev * lax.axis_size("sp")
    reach = WIN_ROWS // 2
    query = triple[..., :local_cols].reshape(samples, rows_dev, GRID_W, local_cols)
    pair = triple[..., local_cols:].reshape(samples, rows_dev, GRID_W, 2 * local_cols)
    padded_pair = extended(pair, (("sp", 1),), reach)
    mixed = attention(query, padded_pair, ctx_pair[None], rel_bias, ctx_bias)
    attended = mixed.reshape(samples, tokens_sp, local_cols)
    attended = attended.transpose(1, 0, 2)
    update = lax.psum_scatter(
        jnp.einsum("tsc,cd->tsd", attended, w_out, preferred_element_type=jnp.float32).astype(
            jnp.bfloat16
        ),
        "tp",
        scatter_dimension=0,
        tiled=True,
    ).astype(jnp.float32)
    gate = modulation[2, :samples, None, :]
    result = latent.astype(jnp.float32) + gate * update.transpose(1, 0, 2)
    return result.astype(jnp.bfloat16)


MESH = pl.DeviceIdType.MESH


def entry_barrier(peers):
    barrier = pltpu.get_barrier_semaphore()
    for device, there in peers:
        @pl.when(there)
        def _():
            pl.semaphore_signal(barrier, inc=1, device_id=device, device_id_type=MESH)
    pl.semaphore_wait(barrier, sum(jnp.where(there, 1, 0) for _, there in peers))


def front_kernel(
    ada_ref, ws_ref, wc_ref, wg_ref, gain_ref, latent_ref, ctx_ref, wq_ref, wk_ref, wv_ref,
    full_ref, q_ref, kv_ref, ckv_ref,
    part, got, total, full, buf, wq, wkv, own_sem, s1, r1, s2, r2, s_ext, r_ext, s_ctx, r_ctx, r_sib,
):
    sp, tp = lax.axis_index("sp"), lax.axis_index("tp")
    n_sp, n_tp = lax.axis_size("sp"), lax.axis_size("tp")
    cols = part.shape[1]
    over_sp = [lax.rem(sp + k, n_sp) for k in range(1, n_sp)]
    over_tp = [lax.rem(tp + k, n_tp) for k in range(1, n_tp)]
    always = sp >= 0
    y, c = tp // 2, lax.rem(tp, 2)
    z, x = sp // 2, lax.rem(sp, 2)
    n_z = n_sp // 2
    sib, across = y * 2 + 1 - c, (1 - y) * 2 + c
    has_up, has_down = sp > 0, sp < n_sp - 1
    direct = y * c + (1 - y) * (6 + c)
    indirect = (1 - y) * c + y * (6 + c)
    has_direct = ((y == 1) & has_up) | ((y == 0) & has_down)
    has_indirect = ((y == 0) & has_up) | ((y == 1) & has_down)
    toward = sp + 2 * y - 1
    here, there = (sp, sib), (sp, across)
    own_slot, across_slot = 2 + tp, 2 + across
    x_peer = sp + 1 - 2 * x
    beside, up, down = (x_peer, tp), (sp + 2, tp), (sp - 2, tp)
    can_up, can_down = sp + 2 < n_sp, sp >= 2
    half = buf.shape[1] // 2
    part_of = pl.ds(pl.multiple_of(c * half, half), half)

    locals_ = [
        pltpu.make_async_copy(wq_ref, wq, own_sem.at[0]),
        pltpu.make_async_copy(wk_ref, wkv.at[:, pl.ds(0, cols)], own_sem.at[1]),
        pltpu.make_async_copy(wv_ref, wkv.at[:, pl.ds(cols, cols)], own_sem.at[2]),
    ]
    for copy in locals_:
        copy.start()
    own_copies = [
        pltpu.make_async_copy(latent_ref.at[s], buf.at[2 * own_slot + s], own_sem.at[3 + s])
        for s in range(2)
    ] + [
        pltpu.make_async_copy(ctx_ref.at[s], buf.at[16 + sp, pl.ds(half * s, half)], own_sem.at[5 + s])
        for s in range(2)
    ]
    for copy in own_copies:
        copy.start()
    entry_barrier([((p, tp), always) for p in over_sp] + [((sp, p), always) for p in over_tp])

    early = []
    mode = ["start"]

    def send(cond, copy):
        @pl.when(cond)
        def _():
            if mode[0] == "start":
                copy.start()
            else:
                copy.wait_send()

    def begin(cond, copy):
        early.append((cond, copy))
        send(cond, copy)

    def arrived(cond, copy):
        if mode[0] == "start":
            @pl.when(cond)
            def _():
                copy.wait_recv()

    def piece(flow, s, device, slot, own=False):
        return pltpu.make_async_remote_copy(
            src_ref=latent_ref.at[s] if own else buf.at[2 * slot + s],
            dst_ref=buf.at[2 * slot + s],
            send_sem=s_ext.at[flow, s], recv_sem=r_ext.at[flow, s],
            device_id=device, device_id_type=MESH,
        )

    def block(at, way, device, own=False):
        return pltpu.make_async_remote_copy(
            src_ref=ctx_ref.at[c] if own else buf.at[16 + at, part_of],
            dst_ref=buf.at[16 + at, part_of],
            send_sem=s_ctx.at[at, way], recv_sem=(r_sib if way == 3 else r_ctx).at[at],
            device_id=device, device_id_type=MESH,
        )

    def first(k, peer):
        return pltpu.make_async_remote_copy(
            src_ref=part, dst_ref=got.at[k], send_sem=s1.at[k], recv_sem=r1.at[k],
            device_id=(peer, tp), device_id_type=MESH,
        )

    columns = pl.ds(pl.multiple_of(tp * cols, cols), cols)

    def second(k, peer):
        return pltpu.make_async_remote_copy(
            src_ref=total, dst_ref=full.at[:, columns], send_sem=s2.at[k], recv_sem=r2.at[k],
            device_id=(sp, peer), device_id_type=MESH,
        )

    for at, weight in enumerate((ws_ref, wc_ref, wg_ref)):
        value = jnp.dot(ada_ref[...], weight[...], preferred_element_type=jnp.float32)
        part[8 * at : 8 * at + 8, :] = value[:8]
    firsts = [first(k, peer) for k, peer in enumerate(over_sp)]
    for copy in firsts:
        copy.start()
    begin(always, piece(1, 0, there, own_slot, True))
    begin(always, block(sp, 0, beside, True))
    begin(can_up, block(sp, 1, up, True))
    begin(can_down, block(sp, 2, down, True))
    for s in range(2):
        begin(has_indirect, piece(2, s, (toward, tp), direct, True))
    for s in range(2):
        begin(always, piece(0, s, here, own_slot, True))
    value = part[...]
    for k, copy in enumerate(firsts):
        copy.wait()
        value = value + got[k]
    total[...] = value
    seconds = [second(k, peer) for k, peer in enumerate(over_tp)]
    for copy in seconds:
        copy.start()
    begin(always, piece(1, 1, there, own_slot, True))
    full[:, columns] = value
    for copy in locals_ + own_copies:
        copy.wait()
    for copy in seconds:
        copy.wait()
    full_ref[...] = full[...]

    def neighbour_block():
        arrived(always, block(x_peer, 0, beside))
        send((c == 0) & can_up, block(x_peer, 1, up))
        send((c == 0) & can_down, block(x_peer, 2, down))
        send(always, block(x_peer, 3, here))

    def relay(hop):
        for e in range(2):
            straight = (c == 0) | (x == e)
            crossing = (c == 1) & (x == e)
            low, high = sp - x - 2 * hop + e, sp - x + 2 * hop + e
            for at, way, device, can, there_is in (
                (lax.max(low, 0), 1, up, can_up, low >= 0),
                (lax.min(high, n_sp - 1), 2, down, can_down, high < n_sp),
            ):
                arrived(there_is, block(at, way, device))
                send(there_is & can & straight, block(at, way, device))
                send(there_is & crossing, block(at, 0, beside))
                send(there_is, block(at, 3, here))

    def from_across(s):
        arrived(always, piece(1, s, there, across_slot))
        send(always, piece(3, s, here, across_slot))

    def from_direct(s):
        arrived(has_direct, piece(2, s, here, direct))
        send(has_direct, piece(5, s, there, direct))
        send(has_direct, piece(6, s, here, direct))

    def from_indirect(s):
        arrived(has_indirect, piece(5, s, there, indirect))
        send(has_indirect, piece(7, s, here, indirect))

    def sibling(flow, s, cond=always):
        arrived(cond, piece(flow, s, here, own_slot))

    def far_block(h, e):
        zb = lax.rem(z + h, n_z)
        at = 2 * zb + e
        arrived(always, block(at, 3, here))

    plan = []

    def add(kind, s, events, at=0):
        plan.append((kind, s, events, at))

    both = lambda flow, cond=always: [functools.partial(sibling, flow, e, cond) for e in range(2)]
    add(0, 0, [])
    add(1, 0, [neighbour_block] + both(0))
    from_peer = lambda: arrived(always, block(x_peer, 3, here))
    add(8, 0, [functools.partial(from_across, 0), functools.partial(from_direct, 0), from_peer], 2 * z)
    add(2, 0, [functools.partial(relay, 1), functools.partial(from_across, 1)])
    add(4, 0, [functools.partial(from_direct, 1)])
    add(3, 0, [functools.partial(relay, 2)] + both(3))
    add(5, 0, both(6, has_direct))
    hops = [functools.partial(relay, hop) for hop in range(3, n_z)]
    for h in range(1, n_z):
        waits = [functools.partial(far_block, h, e) for e in range(2)]
        add(8, 0, (hops + [functools.partial(from_indirect, 0)] if h == 1 else []) + waits, 2 * lax.rem(z + h, n_z))
    add(6, 0, [functools.partial(from_indirect, 1)])
    add(7, 0, both(7, has_indirect))

    slots = (own_slot, 2 + sib, across_slot, 2 + (1 - y) * 2 + 1 - c,
             direct, direct + 1 - 2 * c, indirect, indirect + 1 - 2 * c)

    def step(i, carry):
        at = 0
        row = 0
        exists = 0
        wants = 0
        for k, (kind, s, events, ctx_at) in enumerate(plan):
            on = jnp.where(i == k, 1, 0)
            at = at + on * (16 + ctx_at if kind == 8 else 2 * slots[kind])
            row = row + on * (1 if kind == 8 else 0)
            there_is = has_direct if kind in (4, 5) else has_indirect if kind in (6, 7) else always
            exists = exists + on * jnp.where(there_is, 1, 0)
            wants = wants + on * (1 if kind < 4 else 0)
            if events:
                @pl.when(i == k)
                def _():
                    for event in events:
                        event()

        @pl.when(exists == 1)
        def _():
            hidden = []
            for e in range(2):
                rows = buf[at + e].astype(jnp.float32)
                inverse = lax.rsqrt(jnp.mean(rows * rows, axis=-1, keepdims=True) + EPSILON)
                which = e + row * (2 - e)
                lift = gain_ref[...] * (1.0 + full[pl.ds(8 + which, 1), :])
                rows = rows * inverse * lift + full[pl.ds(which, 1), :]
                hidden.append(rows.astype(jnp.bfloat16))
            hidden = jnp.concatenate(hidden, axis=0)
            count = hidden.shape[0] // 2
            pair = jnp.dot(hidden, wkv[...], preferred_element_type=jnp.float32).astype(jnp.bfloat16)

            @pl.when(at < 16)
            def _():
                for e in range(2):
                    kv_ref[lax.div(lax.min(at, 14), 2) + 8 * e] = pair[e * count : (e + 1) * count]

            @pl.when(at >= 16)
            def _():
                for e in range(2):
                    ckv_ref[lax.max(at - 16, 0) + e] = pair[e * count : (e + 1) * count]

            @pl.when(wants == 1)
            def _():
                query = jnp.dot(hidden, wq[...], preferred_element_type=jnp.float32)
                query = query.astype(jnp.bfloat16)
                for e in range(2):
                    place = lax.div(lax.min(lax.max(at - 4, 0), 6), 2) + 4 * e
                    q_ref[place] = query[e * count : (e + 1) * count]

        @pl.when(exists == 0)
        def _():
            for e in range(2):
                kv_ref[lax.div(lax.min(at, 14), 2) + 8 * e] = jnp.zeros(kv_ref.shape[1:], jnp.bfloat16)

        return carry

    lax.fori_loop(0, len(plan), step, 0)
    mode[0] = "drain"
    for cond, copy in early:
        send(cond, copy)
    for _, _, events, _ in plan:
        for event in events:
            event()


def front(ada_rows, mods, gain, latent, context, w_query, w_key, w_value):
    n_sp, n_tp = lax.axis_size("sp"), lax.axis_size("tp")
    samples, tokens, width = latent.shape
    cols = w_query.shape[1]
    block = (24, cols)
    ada_rows = jnp.pad(ada_rows, ((0, 16 - ada_rows.shape[0]), (0, 0)))
    vmem, hbm = pl.BlockSpec(memory_space=pltpu.VMEM), pl.BlockSpec(memory_space=pl.ANY)
    dma = pltpu.SemaphoreType.DMA
    return pl.pallas_call(
        front_kernel,
        out_shape=(
            jax.ShapeDtypeStruct((24, width), jnp.float32),
            jax.ShapeDtypeStruct((samples * n_tp, tokens, cols), jnp.bfloat16),
            jax.ShapeDtypeStruct((samples * 8, tokens, 2 * cols), jnp.bfloat16),
            jax.ShapeDtypeStruct((n_sp, samples * context.shape[1], 2 * cols), jnp.bfloat16),
        ),
        in_specs=[vmem] * 7 + [hbm] * 3,
        out_specs=[vmem] * 4,
        scratch_shapes=[
            pltpu.VMEM(block, jnp.float32),
            pltpu.VMEM((n_sp - 1,) + block, jnp.float32),
            pltpu.VMEM(block, jnp.float32),
            pltpu.VMEM((24, width), jnp.float32),
            pltpu.VMEM((16 + n_sp, tokens, width), jnp.bfloat16),
            pltpu.VMEM((width, cols), jnp.bfloat16),
            pltpu.VMEM((width, 2 * cols), jnp.bfloat16),
            dma((7,)), dma((n_sp - 1,)), dma((n_sp - 1,)), dma((n_tp - 1,)), dma((n_tp - 1,)),
            dma((8, 2)), dma((8, 2)), dma((n_sp, 4)), dma((n_sp,)), dma((n_sp,)),
        ],
        compiler_params=pltpu.CompilerParams(
            collective_id=1, has_side_effects=True, vmem_limit_bytes=60 * 2**20
        ),
    )(ada_rows, *mods, gain[None, :], latent, context, w_query, w_key, w_value)


def scatter_kernel(parts_ref, out_ref, got, summed, far, s1, r1, s2, r2):
    sp, tp = lax.axis_index("sp"), lax.axis_index("tp")
    y, c = tp // 2, lax.rem(tp, 2)
    sib, across = y * 2 + 1 - c, (1 - y) * 2 + c
    sib_across = (1 - y) * 2 + 1 - c
    entry_barrier([((sp, sib), sp >= 0), ((sp, across), sp >= 0)])
    chunks = far.shape[0]
    rows = far.shape[1]

    def near(k):
        at = k % chunks
        target = sib_across if k < chunks else sib
        return pltpu.make_async_remote_copy(
            src_ref=parts_ref.at[target, pl.ds(at * rows, rows)],
            dst_ref=got.at[k],
            send_sem=s1.at[k], recv_sem=r1.at[k],
            device_id=(sp, sib), device_id_type=MESH,
        )

    def cross(k):
        return pltpu.make_async_remote_copy(
            src_ref=summed.at[k],
            dst_ref=far.at[k],
            send_sem=s2.at[k], recv_sem=r2.at[k],
            device_id=(sp, across), device_id_type=MESH,
        )

    for k in range(2 * chunks):
        near(k).start()
    for k in range(chunks):
        near(k).wait()
        mine = parts_ref[across, k * rows : (k + 1) * rows, :].astype(jnp.float32)
        summed[k] = (mine + got[k].astype(jnp.float32)).astype(jnp.bfloat16)
        cross(k).start()
    for k in range(chunks):
        near(chunks + k).wait()
        cross(k).wait()
        mine = parts_ref[tp, k * rows : (k + 1) * rows, :].astype(jnp.float32)
        mine = mine + got[chunks + k].astype(jnp.float32) + far[k].astype(jnp.float32)
        out_ref[k * rows : (k + 1) * rows, :] = mine


def scatter_sum(parts):
    _, tokens, width = parts.shape
    chunks = 4
    rows = tokens // chunks
    sems = [pltpu.SemaphoreType.DMA((2 * chunks,))] * 2 + [pltpu.SemaphoreType.DMA((chunks,))] * 2
    return pl.pallas_call(
        scatter_kernel,
        out_shape=jax.ShapeDtypeStruct((tokens, width), jnp.float32),
        in_specs=[pl.BlockSpec(memory_space=pltpu.VMEM)],
        out_specs=pl.BlockSpec(memory_space=pltpu.VMEM),
        scratch_shapes=[
            pltpu.VMEM((2 * chunks, rows, width), jnp.bfloat16),
            pltpu.VMEM((chunks, rows, width), jnp.bfloat16),
            pltpu.VMEM((chunks, rows, width), jnp.bfloat16),
        ]
        + sems,
        compiler_params=pltpu.CompilerParams(
            collective_id=3, has_side_effects=True, vmem_limit_bytes=40 * 2**20
        ),
    )(parts)


def on_four(
    latent, context, cond, ctx_cond, w_shift, w_scale, w_gate, norm_gain,
    w_query, w_key, w_value, w_out, rel_bias, ctx_bias,
):
    samples, tokens, width = latent.shape
    n_sp, n_tp = lax.axis_size("sp"), lax.axis_size("tp")
    rows_sp, local_cols = w_shift.shape
    sp = lax.axis_index("sp")
    ada = silu_rows(jnp.concatenate([cond, ctx_cond[None, :]], axis=0))
    ada_rows = lax.dynamic_slice_in_dim(ada, sp * rows_sp, rows_sp, 1)
    modulation, query, pair, ctx_pair = front(
        ada_rows, (w_shift, w_scale, w_gate), norm_gain, latent, context, w_query, w_key, w_value
    )
    modulation = modulation.reshape(3, 8, width)
    rows_dev = n_tp * tokens // GRID_W
    query = query.reshape(samples, rows_dev, GRID_W, local_cols)
    pair = pair.reshape(samples, 2 * rows_dev, GRID_W, 2 * local_cols)
    ctx_pair = ctx_pair.reshape(n_sp, samples, -1, 2 * local_cols)
    mixed = attention(query, pair, ctx_pair, rel_bias, ctx_bias)
    attended = mixed.reshape(samples, n_tp, tokens, local_cols)
    attended = attended.transpose(1, 0, 2, 3).reshape(n_tp, samples * tokens, local_cols)
    parts = jnp.dot(attended, w_out, preferred_element_type=jnp.float32).astype(jnp.bfloat16)
    update = scatter_sum(parts).reshape(samples, tokens, width)
    gate = modulation[2, :samples, None, :]
    return (latent.astype(jnp.float32) + gate * update).astype(jnp.bfloat16)


def solution(mesh):
    shape = dict(mesh.shape)
    quick = shape["tp"] == 4 and shape["sp"] == 8
    return jax.shard_map(
        on_four if quick else on_device,
        mesh=mesh,
        in_specs=(
            P(None, ("sp", "tp"), None),
            P(None, "sp", None),
            P(),
            P(),
            P("sp", "tp"),
            P("sp", "tp"),
            P("sp", "tp"),
            P(),
            P(None, "tp"),
            P(None, "tp"),
            P(None, "tp"),
            P("tp", None),
            P("tp", None, None),
            P("tp"),
        ),
        out_specs=P(None, ("sp", "tp"), None),
        check_vma=False,
    )
```
